32 devices in a mesh: kv: 8 (over z, y), tp: 4 (over x, core).
Axes of the slice: x: 2, y: 2, z: 4, core: 2. Of those that a mesh axis runs over, the one named last changes fastest.
Arguments:
- tokens: bfloat16 [16, 4096], P(None, 'tp'), may hold values from -6 to 6
- norm_gain: float32 [4096], P('tp'), may hold values from 0.1 to 1.9
- w_query: bfloat16 [4096, 32, 96], P('tp', 'kv'), as said below
- w_latent: bfloat16 [4096, 1024], P('tp', 'kv'), may hold values from -0.09375 to 0.09375
- w_rotary: bfloat16 [4096, 32], P('tp'), may hold values from -0.09375 to 0.09375
- latent_gain: float32 [1024], replicated, may hold values from 0.1 to 1.9
- w_key_up: bfloat16 [1024, 32, 64], P('tp', 'kv'), may hold values from -0.1875 to 0.1875
- w_value_up: bfloat16 [1024, 32, 128], replicated, may hold values from -0.1875 to 0.1875
- w_out: bfloat16 [4096, 4096], P('kv', 'tp'), may hold values from -0.09375 to 0.09375
- cache_latent: bfloat16 [16, 4096, 1024], P(None, ('kv', 'tp')), may hold values from -6 to 6
- cache_rotary: bfloat16 [16, 4096, 32], P(None, ('kv', 'tp')), may hold values from -6 to 6
- lengths: int32 [16], replicated, may hold values from 1024 to 4096
Outputs:
- mixed_out: bfloat16 [16, 4096], P(None, 'tp')
- new_latent: bfloat16 [16, 1024], P(None, ('kv', 'tp'))
- new_rotary: bfloat16 [16, 32], replicated
The draws below stay inside these ranges and needn't reach their ends.
Inputs may be any that keep to these rules, and one draw needn't show every extreme that they name: `w_query`: finite.
All inputs are finite; a program needn't handle non-finite values.
Results may differ from the reference program's by a relative error of at most 0.012.
The reference program's roundings to bfloat16 on the way count: a program that leaves them out, or rounds other values in their place, can miss the bound.
Values may be sent and summed in bfloat16 or wider, within the bound.
A program may use at most 64 MiB of HBM per device.

```python
import jax
import jax.numpy as jnp
from jax import lax

D = 4096
HEADS = 32
NOPE = 64
ROPE = 32
VH = 128
LATENT = 1024
SEQS = 16
CACHE = 4096


def draw_w_query(key, part):
    base_key = jax.random.fold_in(key, 11)
    pick_key = jax.random.fold_in(key, 12)
    order = jax.random.permutation(pick_key, HEADS)
    values = jax.random.truncated_normal(base_key, -6.0, 6.0, (D, HEADS, NOPE + ROPE), jnp.float32) * D ** (-0.5)
    strengths = jnp.array([30.0, 60.0], jnp.float32)
    factor = jnp.full((HEADS,), 5.0, jnp.float32)
    factor = factor.at[order[:strengths.shape[0]]].set(strengths)
    return (values * factor[None, :, None]).astype(jnp.bfloat16)


def touch_ends(result, key, smallest, high):
    longest = result.shape.index(max(result.shape))
    spots = []
    for shift in (0, 1):
        where = [jax.random.randint(jax.random.fold_in(key, axis), (), 0, length) for axis, length in enumerate(result.shape)]
        where[longest] = (where[longest] + shift) % result.shape[longest]
        spots.append(tuple(where))
    return result.at[spots[0]].set(smallest).at[spots[1]].set(high)


def block_levels(rng, dims, split, low, largest):
    def one(dim, shards_of):
        heights = jax.random.uniform(jax.random.fold_in(jax.random.fold_in(rng, 6), dim), (shards_of,), jnp.float32, low / len(split), largest / len(split))
        return jnp.repeat(jnp.exp(heights), dims[dim] // shards_of).reshape((-1,) + (1,) * (len(dims) - dim - 1))

    level = one(*split[0])
    for cut in split[1:]:
        level = level * one(*cut)
    return level


def gaussian(key, shape, spread, bound, shards=(), kind=jnp.bfloat16):
    result = jax.random.normal(key, shape, jnp.float32) * spread
    if len(shards) > 0:
        result = block_levels(key, shape, shards, -0.22, 0.18) * result
    return jnp.clip(result, min=-bound, max=bound).astype(kind)


def setup_inputs(seed: int = 0) -> dict:
    splits = jax.random.split(jax.random.key(seed), 13)
    return {
        "tokens": gaussian(splits[0], (SEQS, D), 1.0, 6.0, ((1, 4),)),
        "norm_gain": jnp.clip(1.0 + 0.18 * jax.random.normal(splits[1], (D,), jnp.float32), 0.1, 1.9),
        "w_query": draw_w_query(jax.random.fold_in(splits[12], 71), 0),
        "w_latent": gaussian(splits[3], (D, LATENT), D ** -0.5, 0.09375, ((0, 4), (1, 8))),
        "w_rotary": gaussian(splits[4], (D, ROPE), D ** -0.5, 0.09375, ((0, 4),)),
        "latent_gain": jnp.clip(1.0 + 0.18 * jax.random.normal(splits[5], (LATENT,), jnp.float32), 0.1, 1.9),
        "w_key_up": gaussian(splits[6], (LATENT, HEADS, NOPE), LATENT ** -0.5, 0.1875, ((0, 4), (1, 8))),
        "w_value_up": gaussian(splits[7], (LATENT, HEADS, VH), LATENT ** -0.5, 0.1875),
        "w_out": gaussian(splits[8], (HEADS * VH, D), (HEADS * VH) ** -0.5, 0.09375, ((0, 8), (1, 4))),
        "cache_latent": gaussian(splits[9], (SEQS, CACHE, LATENT), 1.0, 6.0, ((1, 32),)),
        "cache_rotary": gaussian(splits[10], (SEQS, CACHE, ROPE), 1.0, 6.0, ((1, 32),)),
        "lengths": touch_ends(jax.random.randint(splits[11], (SEQS,), CACHE // 4, CACHE + 1), jax.random.fold_in(splits[11], 1), CACHE // 4, CACHE).astype(jnp.int32),
    }


THETA = 10000.0
EPS = 1e-06

def rotate(values, position):
    full_width = values.shape[-1]
    half_width = full_width // 2
    frequency = THETA ** (-jnp.arange(0, full_width, 2, dtype=jnp.float32) / full_width)
    angles = position.astype(jnp.float32)[:, None] * frequency[None, :]
    angles = angles.reshape((angles.shape[0],) + (1,) * (values.ndim - 2) + (half_width,))
    cosine = jnp.cos(angles)
    sine_part = jnp.sin(angles)
    first_half = values[..., :half_width]
    second_half = values[..., half_width:]
    return jnp.concatenate([first_half * cosine - second_half * sine_part, first_half * sine_part + second_half * cosine], axis=-1)

def reference(tokens, norm_gain, w_query, w_latent, w_rotary, latent_gain, w_key_up, w_value_up, w_out, cache_latent, cache_rotary, lengths):
    tokens_f = tokens.astype(jnp.float32)
    scaled = (tokens_f * norm_gain).astype(jnp.bfloat16)
    inverse = lax.rsqrt(lax.optimization_barrier(jnp.mean(tokens_f * tokens_f, axis=1)) + EPS)
    query_sum = jnp.einsum('bd,dhn->bhn', scaled.astype(jnp.float32), w_query.astype(jnp.float32))
    latent_sum = jnp.dot(scaled, w_latent, preferred_element_type=jnp.float32)
    rotary_sum = jnp.dot(scaled, w_rotary, preferred_element_type=jnp.float32)
    query_heads = (query_sum * inverse[:, None, None]).astype(jnp.bfloat16)
    compressed = (latent_sum * inverse[:, None]).astype(jnp.bfloat16)
    new_rotary = rotate(rotary_sum * inverse[:, None], lengths).astype(jnp.bfloat16)
    query_rope = rotate(query_heads[:, :, NOPE:].astype(jnp.float32), lengths).astype(jnp.bfloat16)
    query_latent = jnp.einsum('bhn,rhn->bhr', query_heads[:, :, :NOPE].astype(jnp.float32), w_key_up.astype(jnp.float32)).astype(jnp.bfloat16)
    compressed_f = compressed.astype(jnp.float32)
    new_latent = (compressed_f * lax.rsqrt(lax.optimization_barrier(jnp.mean(compressed_f * compressed_f, axis=1, keepdims=True)) + EPS) * latent_gain).astype(jnp.bfloat16)
    score_scale = (NOPE + ROPE) ** (-0.5)
    own_score = (jnp.einsum('bhr,br->bh', query_latent.astype(jnp.float32), new_latent.astype(jnp.float32)) + jnp.einsum('bhq,bq->bh', query_rope.astype(jnp.float32), new_rotary.astype(jnp.float32))) * score_scale

    def attend(items):
        latent_query, rope_query, past_latent, past_rotary, length, own, fresh = items
        scores = (jnp.dot(latent_query, past_latent.T, preferred_element_type=jnp.float32) + jnp.dot(rope_query, past_rotary.T, preferred_element_type=jnp.float32)) * score_scale
        valid = jnp.arange(CACHE, dtype=jnp.int32) < length
        masked = jnp.where(valid[None, :], scores, -jnp.inf)
        top_score = jnp.maximum(lax.optimization_barrier(jnp.max(masked, axis=1)), own)
        weights = jnp.where(valid[None, :], jnp.exp(scores - top_score[:, None]), 0.0)
        own_weight = jnp.exp(own - top_score)
        total = lax.optimization_barrier(jnp.sum(weights, axis=1)) + own_weight
        summed = jnp.dot(weights.astype(jnp.bfloat16), past_latent, preferred_element_type=jnp.float32)
        summed = summed + own_weight[:, None] * fresh.astype(jnp.float32)[None, :]
        return summed / total[:, None]
    latent_out = lax.map(attend, (query_latent, query_rope, cache_latent, cache_rotary, lengths, own_score, new_latent))
    head_out = jnp.einsum('bhr,rhv->bhv', latent_out, w_value_up.astype(jnp.float32), precision=lax.Precision.HIGHEST).astype(jnp.bfloat16)
    mixed_out = jnp.dot(head_out.reshape(head_out.shape[0], -1), w_out, preferred_element_type=jnp.float32).astype(jnp.bfloat16)
    return (mixed_out, new_latent, new_rotary)
```

```python
import functools

import jax
import jax.numpy as jnp
from jax import lax
from jax.experimental import pallas as pl
from jax.experimental.pallas import tpu as pltpu
from jax.sharding import PartitionSpec as P

MESH = pl.DeviceIdType.MESH
LANES = 128

THETA = 10000.0
EPS = 1e-06


def rotate(values, position):
    full_width = values.shape[-1]
    half_width = full_width // 2
    frequency = THETA ** (-jnp.arange(0, full_width, 2, dtype=jnp.float32) / full_width)
    angles = position.astype(jnp.float32)[:, None] * frequency[None, :]
    angles = angles.reshape((angles.shape[0],) + (1,) * (values.ndim - 2) + (half_width,))
    cosine = jnp.cos(angles)
    sine_part = jnp.sin(angles)
    first_half = values[..., :half_width]
    second_half = values[..., half_width:]
    return jnp.concatenate(
        [
            first_half * cosine - second_half * sine_part,
            first_half * sine_part + second_half * cosine,
        ],
        axis=-1,
    )


def value_product(latent_f, weight):
    high_part = latent_f.astype(jnp.bfloat16)
    low_part = (latent_f - high_part.astype(jnp.float32)).astype(jnp.bfloat16)
    return jnp.einsum(
        "bhr,rhv->bhv", high_part, weight, preferred_element_type=jnp.float32
    ) + jnp.einsum("bhr,rhv->bhv", low_part, weight, preferred_element_type=jnp.float32)


def greet(peers):
    barrier = pltpu.get_barrier_semaphore()
    for peer in peers:
        pl.semaphore_signal(barrier, inc=1, device_id=peer, device_id_type=MESH)
    pl.semaphore_wait(barrier, len(peers))


def remote(source, target, send, recv, peer):
    return pltpu.make_async_remote_copy(
        src_ref=source,
        dst_ref=target,
        send_sem=send,
        recv_sem=recv,
        device_id=peer,
        device_id_type=MESH,
    )


def tp_sum_kernel(tp_count, part_ref, sum_ref, slots, send, recv):
    kv_index, tp_index = lax.axis_index("kv"), lax.axis_index("tp")
    peers = [(kv_index, lax.rem(tp_index + step, tp_count)) for step in range(1, tp_count)]
    greet(peers)
    copies = []
    for step, peer in enumerate(peers):
        copies.append(
            remote(part_ref, slots.at[tp_index], send.at[step], recv.at[step], peer)
        )
        copies[-1].start()
    slots[tp_index] = part_ref[...]
    for copy in copies:
        copy.wait()
    sum_ref[...] = jnp.sum(slots[...], axis=0)


def tp_sum(part, tp_count):
    return pl.pallas_call(
        functools.partial(tp_sum_kernel, tp_count),
        out_shape=jax.ShapeDtypeStruct(part.shape, part.dtype),
        in_specs=[pl.BlockSpec(memory_space=pltpu.VMEM)],
        out_specs=pl.BlockSpec(memory_space=pltpu.VMEM),
        scratch_shapes=[
            pltpu.VMEM((tp_count,) + part.shape, part.dtype),
            pltpu.SemaphoreType.DMA((tp_count - 1,)),
            pltpu.SemaphoreType.DMA((tp_count - 1,)),
        ],
        compiler_params=pltpu.CompilerParams(collective_id=0, has_side_effects=True),
        name="tp_sum",
    )(part)


def chip_offsets(kv_count, tp_count):
    return [
        (kv_step, tp_step)
        for kv_step in range(kv_count)
        for tp_step in range(0, tp_count, 2)
        if kv_step + tp_step > 0
    ]


def sibling_of(tp_index):
    return tp_index + 1 - 2 * lax.rem(tp_index, 2)


def gather_kernel(
    kv_count,
    tp_count,
    query_ref,
    extra_ref,
    query_out,
    extra_out,
    query_all,
    extra_all,
    chip_send,
    chip_recv,
    pair_send,
    pair_recv,
    extra_send,
    extra_recv,
):
    kv_index, tp_index = lax.axis_index("kv"), lax.axis_index("tp")
    heads, _, width = query_ref.shape
    offsets = chip_offsets(kv_count, tp_count)
    sibling = (kv_index, sibling_of(tp_index))
    greet(
        [
            (lax.rem(kv_index + kv_step, kv_count), lax.rem(tp_index + tp_step, tp_count))
            for kv_step, tp_step in offsets
        ]
        + [sibling]
    )

    def place(kv_at, tp_at):
        return query_all.at[
            pl.ds(pl.multiple_of(kv_at * heads, heads), heads),
            :,
            pl.ds(pl.multiple_of(tp_at * width, LANES), width),
        ]

    mine = place(kv_index, tp_index)
    chip_copies, pair_copies, extra_copies = [], [], []
    for slot, (kv_step, tp_step) in enumerate(offsets):
        peer = (lax.rem(kv_index + kv_step, kv_count), lax.rem(tp_index + tp_step, tp_count))
        chip_copies.append(remote(query_ref, mine, chip_send.at[slot], chip_recv.at[slot], peer))
        chip_copies[-1].start()
        if tp_step == 0:
            extra_copies.append(
                remote(
                    extra_ref,
                    extra_all.at[kv_index],
                    extra_send.at[kv_step - 1],
                    extra_recv.at[kv_step - 1],
                    peer,
                )
            )
            extra_copies[-1].start()
    last = len(offsets)
    pair_copies.append(remote(query_ref, mine, pair_send.at[last], pair_recv.at[last], sibling))
    pair_copies[-1].start()
    query_all[
        pl.ds(pl.multiple_of(kv_index * heads, heads), heads),
        :,
        pl.ds(pl.multiple_of(tp_index * width, LANES), width),
    ] = query_ref[...]
    extra_all[kv_index] = extra_ref[...]
    for slot, (kv_step, tp_step) in enumerate(offsets):
        chip_copies[slot].wait_recv()
        block = place(
            lax.rem(kv_index - kv_step + kv_count, kv_count),
            lax.rem(tp_index - tp_step + tp_count, tp_count),
        )
        pair_copies.append(remote(block, block, pair_send.at[slot], pair_recv.at[slot], sibling))
        pair_copies[-1].start()
    for copy in extra_copies:
        copy.wait()
    for copy in chip_copies:
        copy.wait_send()
    for copy in pair_copies:
        copy.wait()
    query_out[...] = query_all[...]
    extra_out[...] = extra_all[...]


def gather_all(query, extra, kv_count, tp_count):
    heads, seqs, width = query.shape
    query_shape = (heads * kv_count, seqs, width * tp_count)
    extra_shape = (kv_count,) + extra.shape
    chips = kv_count * tp_count // 2
    return pl.pallas_call(
        functools.partial(gather_kernel, kv_count, tp_count),
        out_shape=(
            jax.ShapeDtypeStruct(query_shape, query.dtype),
            jax.ShapeDtypeStruct(extra_shape, extra.dtype),
        ),
        in_specs=[pl.BlockSpec(memory_space=pltpu.VMEM)] * 2,
        out_specs=(pl.BlockSpec(memory_space=pltpu.VMEM),) * 2,
        scratch_shapes=[
            pltpu.VMEM(query_shape, query.dtype),
            pltpu.VMEM(extra_shape, extra.dtype),
            pltpu.SemaphoreType.DMA((chips - 1,)),
            pltpu.SemaphoreType.DMA((chips - 1,)),
            pltpu.SemaphoreType.DMA((chips,)),
            pltpu.SemaphoreType.DMA((chips,)),
            pltpu.SemaphoreType.DMA((kv_count - 1,)),
            pltpu.SemaphoreType.DMA((kv_count - 1,)),
        ],
        compiler_params=pltpu.CompilerParams(collective_id=1, has_side_effects=True),
        name="gather_all",
    )(query, extra)


def split_stats(block, rank):
    values = block[:, :rank].astype(jnp.float32)
    stats = block[:, rank:].astype(jnp.float32)
    top = (stats[:, 0:1] + stats[:, 1:2]) + stats[:, 2:3]
    return values, top, stats[:, 3:4] + stats[:, 4:5]


def merge(first, second):
    values_a, top_a, total_a = first
    values_b, top_b, total_b = second
    top = jnp.maximum(top_a, top_b)
    scale_a, scale_b = jnp.exp(top_a - top), jnp.exp(top_b - top)
    return values_a * scale_a + values_b * scale_b, top, total_a * scale_a + total_b * scale_b


def rounded(value):
    return lax.reduce_precision(value, 8, 7)


def narrow(value):
    return value.astype(jnp.bfloat16).astype(jnp.float32)


def stats_lanes(top, total, lane, cut):
    high = cut(top)
    middle = cut(top - high)
    low = top - high - middle
    total_high = cut(total)
    total_low = total - total_high
    result = jnp.where(lane == 4, total_low, 0.0)
    for place, value in enumerate((high, middle, low, total_high)):
        result = jnp.where(lane == place, value, result)
    return result


def scatter_kernel(
    kv_count,
    tp_count,
    part_ref,
    sum_ref,
    stats_ref,
    from_pair,
    merged,
    from_chips,
    pair_send,
    pair_recv,
    chip_send,
    chip_recv,
):
    kv_index, tp_index = lax.axis_index("kv"), lax.axis_index("tp")
    rank = sum_ref.shape[1]
    seqs = sum_ref.shape[0]
    lane = lax.broadcasted_iota(jnp.int32, (seqs, LANES), 1)
    offsets = chip_offsets(kv_count, tp_count)
    sibling = (kv_index, sibling_of(tp_index))
    targets = [
        (lax.rem(kv_index + kv_step, kv_count), lax.rem(tp_index + tp_step, tp_count))
        for kv_step, tp_step in offsets
    ]
    greet(targets + [sibling])
    places = targets + [(kv_index, tp_index)]
    pair_copies, chip_copies = [], []
    for slot, (kv_at, tp_at) in enumerate(places):
        pair_copies.append(
            remote(
                part_ref.at[kv_at * tp_count + sibling_of(tp_at)],
                from_pair.at[slot],
                pair_send.at[slot],
                pair_recv.at[slot],
                sibling,
            )
        )
        pair_copies[-1].start()
    own = None
    for slot, (kv_at, tp_at) in enumerate(places):
        pair_copies[slot].wait_recv()
        values, top, total = merge(
            split_stats(part_ref[kv_at * tp_count + tp_at], rank),
            split_stats(from_pair[slot], rank),
        )
        if slot == len(targets):
            own = (values, top, total)
            continue
        merged[slot, :, :rank] = values.astype(merged.dtype)
        merged[slot, :, rank:] = stats_lanes(top, total, lane, narrow).astype(merged.dtype)
        chip_copies.append(
            remote(
                merged.at[slot],
                from_chips.at[slot],
                chip_send.at[slot],
                chip_recv.at[slot],
                targets[slot],
            )
        )
        chip_copies[-1].start()
    for slot, copy in enumerate(chip_copies):
        copy.wait_recv()
        own = merge(own, split_stats(from_chips[slot], rank))
    values, top, total = own
    sum_ref[...] = values
    stats_ref[...] = jnp.where(lane == 0, top, total)
    for copy in chip_copies:
        copy.wait_send()
    for copy in pair_copies:
        copy.wait_send()


def scatter_sum(part, rank, kv_count, tp_count):
    _, seqs, width = part.shape
    chips = kv_count * tp_count // 2
    return pl.pallas_call(
        functools.partial(scatter_kernel, kv_count, tp_count),
        out_shape=(
            jax.ShapeDtypeStruct((seqs, rank), jnp.float32),
            jax.ShapeDtypeStruct((seqs, LANES), jnp.float32),
        ),
        in_specs=[pl.BlockSpec(memory_space=pltpu.VMEM)],
        out_specs=(pl.BlockSpec(memory_space=pltpu.VMEM),) * 2,
        scratch_shapes=[
            pltpu.VMEM((chips, seqs, width), part.dtype),
            pltpu.VMEM((chips - 1, seqs, width), part.dtype),
            pltpu.VMEM((chips - 1, seqs, width), part.dtype),
            pltpu.SemaphoreType.DMA((chips,)),
            pltpu.SemaphoreType.DMA((chips,)),
            pltpu.SemaphoreType.DMA((chips - 1,)),
            pltpu.SemaphoreType.DMA((chips - 1,)),
        ],
        compiler_params=pltpu.CompilerParams(collective_id=2, has_side_effects=True),
        name="scatter_sum",
    )(part)


def out_kernel(
    kv_count,
    tp_count,
    head_ref,
    weight_ref,
    out_ref,
    heads,
    parts,
    got,
    done,
    final,
    head_send,
    head_recv,
    part_send,
    part_recv,
    done_send,
    done_recv,
):
    kv_index, tp_index = lax.axis_index("kv"), lax.axis_index("tp")
    depth = head_ref.shape[1]
    width = parts.shape[2]
    tp_peers = [(kv_index, lax.rem(tp_index + step, tp_count)) for step in range(1, tp_count)]
    kv_peers = [(lax.rem(kv_index + step, kv_count), tp_index) for step in range(1, kv_count)]
    greet(tp_peers + kv_peers)
    copies = []
    for step, peer in enumerate(tp_peers):
        copies.append(
            remote(head_ref, heads.at[tp_index], head_send.at[step], head_recv.at[step], peer)
        )
        copies[-1].start()
    heads[tp_index] = head_ref[...]
    for copy in copies:
        copy.wait()
    total = jnp.dot(heads[0], weight_ref[:depth, :], preferred_element_type=jnp.float32)
    for at in range(1, tp_count):
        total += jnp.dot(
            heads[at],
            weight_ref[at * depth : (at + 1) * depth, :],
            preferred_element_type=jnp.float32,
        )
    for at in range(kv_count):
        parts[at] = total[:, at * width : (at + 1) * width]
    copies = []
    for step, peer in enumerate(kv_peers):
        copies.append(
            remote(
                parts.at[peer[0]],
                got.at[kv_index],
                part_send.at[step],
                part_recv.at[step],
                peer,
            )
        )
        copies[-1].start()
    got[kv_index] = parts[kv_index]
    for copy in copies:
        copy.wait()
    mine = jnp.sum(got[...], axis=0).astype(out_ref.dtype)
    done[...] = mine
    copies = []
    for step, peer in enumerate(kv_peers):
        copies.append(
            remote(done, final.at[kv_index], done_send.at[step], done_recv.at[step], peer)
        )
        copies[-1].start()
    final[kv_index] = mine
    for copy in copies:
        copy.wait()
    for at in range(kv_count):
        out_ref[:, at * width : (at + 1) * width] = final[at]


def project_out(head_out, weight, kv_count, tp_count):
    seqs, depth = head_out.shape
    columns = weight.shape[1]
    width = columns // kv_count
    return pl.pallas_call(
        functools.partial(out_kernel, kv_count, tp_count),
        out_shape=jax.ShapeDtypeStruct((seqs, columns), jnp.bfloat16),
        in_specs=[pl.BlockSpec(memory_space=pltpu.VMEM)] * 2,
        out_specs=pl.BlockSpec(memory_space=pltpu.VMEM),
        scratch_shapes=[
            pltpu.VMEM((tp_count, seqs, depth), head_out.dtype),
            pltpu.VMEM((kv_count, seqs, width), jnp.float32),
            pltpu.VMEM((kv_count, seqs, width), jnp.float32),
            pltpu.VMEM((seqs, width), jnp.bfloat16),
            pltpu.VMEM((kv_count, seqs, width), jnp.bfloat16),
            pltpu.SemaphoreType.DMA((tp_count - 1,)),
            pltpu.SemaphoreType.DMA((tp_count - 1,)),
            pltpu.SemaphoreType.DMA((kv_count - 1,)),
            pltpu.SemaphoreType.DMA((kv_count - 1,)),
            pltpu.SemaphoreType.DMA((kv_count - 1,)),
            pltpu.SemaphoreType.DMA((kv_count - 1,)),
        ],
        compiler_params=pltpu.CompilerParams(collective_id=3, has_side_effects=True),
        name="project_out",
    )(head_out, weight)


def kernel_shards(
    tokens,
    norm_gain,
    w_query,
    w_latent,
    w_rotary,
    latent_gain,
    w_key_up,
    w_value_up,
    w_out,
    cache_latent,
    cache_rotary,
    lengths,
):
    seq_count = tokens.shape[0]
    kv_count = lax.axis_size("kv")
    tp_count = lax.axis_size("tp")
    kv_index = lax.axis_index("kv")
    tp_index = lax.axis_index("tp")
    device = kv_index * tp_count + tp_index
    heads_dev = w_query.shape[1]
    head_count = heads_dev * kv_count
    latent_rank = cache_latent.shape[2]
    rope_width = cache_rotary.shape[2]
    nope_width = w_query.shape[2] - rope_width
    model_width = tokens.shape[1] * tp_count
    score_scale = w_query.shape[2] ** (-0.5)
    tokens_f = tokens.astype(jnp.float32)
    scaled = (tokens_f * norm_gain).astype(jnp.bfloat16)
    query_part = jnp.einsum("bd,dhn->bhn", scaled, w_query, preferred_element_type=jnp.float32)
    latent_part = jnp.dot(scaled, w_latent, preferred_element_type=jnp.float32)
    rotary_part = jnp.dot(scaled, w_rotary, preferred_element_type=jnp.float32)
    square_part = jnp.sum(tokens_f * tokens_f, axis=1)
    query_width = heads_dev * w_query.shape[2]
    latent_width = latent_part.shape[1]
    fill = -(query_width + latent_width + rope_width) % LANES or LANES
    packed = jnp.concatenate(
        [
            query_part.reshape(seq_count, query_width),
            latent_part,
            rotary_part,
            jnp.broadcast_to(square_part[:, None], (seq_count, fill)),
        ],
        axis=1,
    )
    packed = tp_sum(packed, tp_count)
    query_sum, latent_sum, rotary_sum, square_sum = jnp.split(
        packed,
        [query_width, query_width + latent_width, query_width + latent_width + rope_width],
        axis=1,
    )
    inverse = lax.rsqrt(square_sum[:, :1] / model_width + EPS)
    query_heads = (query_sum * inverse).astype(jnp.bfloat16)
    query_heads = query_heads.reshape(seq_count, heads_dev, w_query.shape[2])
    compressed = (latent_sum * inverse).astype(jnp.bfloat16)
    new_rotary = rotate(rotary_sum * inverse, lengths).astype(jnp.bfloat16)
    query_rope = rotate(query_heads[:, :, nope_width:].astype(jnp.float32), lengths).astype(
        jnp.bfloat16
    )
    query_latent = jnp.einsum(
        "bhn,rhn->hbr", query_heads[:, :, :nope_width], w_key_up, preferred_element_type=jnp.float32
    ).astype(jnp.bfloat16)
    rope_flat = query_rope.reshape(seq_count, heads_dev * rope_width)
    got_latent, got_extra = gather_all(
        query_latent, jnp.concatenate([rope_flat, compressed], axis=1), kv_count, tp_count
    )
    all_latent = got_latent.transpose(1, 0, 2)
    all_rope = got_extra[:, :, : heads_dev * rope_width]
    all_rope = all_rope.reshape(kv_count, seq_count, heads_dev, rope_width)
    all_rope = all_rope.transpose(1, 0, 2, 3).reshape(seq_count, head_count, rope_width)
    fresh_f = got_extra[:, :, heads_dev * rope_width :].transpose(1, 0, 2)
    fresh_f = fresh_f.reshape(seq_count, latent_rank).astype(jnp.float32)
    new_latent = (
        fresh_f * lax.rsqrt(jnp.mean(fresh_f * fresh_f, axis=1, keepdims=True) + EPS) * latent_gain
    ).astype(jnp.bfloat16)
    new_latent_f = new_latent.astype(jnp.float32)
    own_score = (
        jnp.einsum("bhr,br->bh", all_latent, new_latent, preferred_element_type=jnp.float32)
        + jnp.einsum("bhq,bq->bh", all_rope, new_rotary, preferred_element_type=jnp.float32)
    ) * score_scale
    pos_dev = cache_latent.shape[1]
    position = device * pos_dev + jnp.arange(pos_dev, dtype=jnp.int32)
    valid = position[None, :] < lengths[:, None]
    scores = (
        jnp.einsum("bhr,bpr->bhp", all_latent, cache_latent, preferred_element_type=jnp.float32)
        + jnp.einsum("bhq,bpq->bhp", all_rope, cache_rotary, preferred_element_type=jnp.float32)
    ) * score_scale
    masked = jnp.where(valid[:, None, :], scores, -jnp.inf)
    local_top = jnp.maximum(jnp.max(masked, axis=2), own_score)
    weights = jnp.where(valid[:, None, :], jnp.exp(scores - local_top[:, :, None]), 0.0)
    total_part = jnp.sum(weights, axis=2)
    summed_part = jnp.einsum(
        "bhp,bpr->bhr",
        weights.astype(jnp.bfloat16),
        cache_latent,
        preferred_element_type=jnp.float32,
    ).astype(jnp.bfloat16)
    lane = lax.broadcasted_iota(jnp.int32, (seq_count, head_count, LANES), 2)
    stats = stats_lanes(local_top[:, :, None], total_part[:, :, None], lane, rounded)
    part = jnp.concatenate([summed_part, stats.astype(jnp.bfloat16)], axis=2).transpose(1, 0, 2)
    block_sum, block_stats = scatter_sum(part, latent_rank, kv_count, tp_count)
    own = lax.dynamic_slice_in_dim(own_score, device, 1, 1)
    block_top, block_total = block_stats[:, 0:1], block_stats[:, 1:2]
    top_score = jnp.maximum(block_top, own)
    old_scale, own_weight = jnp.exp(block_top - top_score), jnp.exp(own - top_score)
    latent_out = (block_sum * old_scale + own_weight * new_latent_f) / (
        block_total * old_scale + own_weight
    )
    value_weight = lax.dynamic_slice_in_dim(w_value_up, device, 1, 1)
    head_out = value_product(latent_out[:, None, :], value_weight).astype(jnp.bfloat16)
    mixed_out = project_out(head_out[:, 0, :], w_out, kv_count, tp_count)
    piece_width = latent_rank // (kv_count * tp_count)
    latent_piece = lax.dynamic_slice_in_dim(new_latent, device * piece_width, piece_width, 1)
    return (mixed_out, latent_piece, new_rotary)


def fits_kernels(args, kv_count, tp_count):
    w_query, w_latent, w_rotary, w_key_up, w_value_up, w_out = args
    heads = w_query.shape[1]
    return (
        heads == kv_count * tp_count
        and tp_count % 2 == 0
        and w_key_up.shape[0] // tp_count % LANES == 0
        and w_latent.shape[1] // kv_count % LANES == 0
        and heads // kv_count * w_rotary.shape[1] % LANES == 0
        and w_value_up.shape[2] % LANES == 0
        and w_out.shape[1] // tp_count // kv_count % LANES == 0
    )


def shards(
    tokens,
    norm_gain,
    w_query,
    w_latent,
    w_rotary,
    latent_gain,
    w_key_up,
    w_value_up,
    w_out,
    cache_latent,
    cache_rotary,
    lengths,
):
    seq_count = tokens.shape[0]
    kv_count = lax.axis_size("kv")
    tp_count = lax.axis_size("tp")
    kv_index = lax.axis_index("kv")
    tp_index = lax.axis_index("tp")
    heads_dev = w_query.shape[1]
    head_count = heads_dev * kv_count
    latent_rank = cache_latent.shape[2]
    rope_width = cache_rotary.shape[2]
    nope_width = w_query.shape[2] - rope_width
    model_width = tokens.shape[1] * tp_count
    score_scale = w_query.shape[2] ** (-0.5)
    tokens_f = tokens.astype(jnp.float32)
    scaled = (tokens_f * norm_gain).astype(jnp.bfloat16)
    query_part = jnp.einsum("bd,dhn->bhn", scaled, w_query, preferred_element_type=jnp.float32)
    latent_part = jnp.dot(scaled, w_latent, preferred_element_type=jnp.float32)
    rotary_part = jnp.dot(scaled, w_rotary, preferred_element_type=jnp.float32)
    square_part = jnp.sum(tokens_f * tokens_f, axis=1)
    query_sum, latent_sum, rotary_sum, square_sum = lax.psum(
        (query_part, latent_part, rotary_part, square_part), "tp"
    )
    inverse = lax.rsqrt(square_sum / model_width + EPS)
    query_heads = (query_sum * inverse[:, None, None]).astype(jnp.bfloat16)
    compressed = (latent_sum * inverse[:, None]).astype(jnp.bfloat16)
    new_rotary = rotate(rotary_sum * inverse[:, None], lengths).astype(jnp.bfloat16)
    query_rope = rotate(query_heads[:, :, nope_width:].astype(jnp.float32), lengths).astype(
        jnp.bfloat16
    )
    query_latent = jnp.einsum(
        "bhn,rhn->bhr", query_heads[:, :, :nope_width], w_key_up, preferred_element_type=jnp.float32
    ).astype(jnp.bfloat16)
    rope_slice = rope_width // tp_count
    column_slice = compressed.shape[1] // tp_count
    rope_piece = lax.dynamic_slice_in_dim(query_rope, tp_index * rope_slice, rope_slice, 2)
    column_piece = lax.dynamic_slice_in_dim(compressed, tp_index * column_slice, column_slice, 1)
    got_latent, got_rope, got_columns = (
        lax.all_gather(query_latent[:, None], ("kv", "tp"), axis=1, tiled=True),
        lax.all_gather(rope_piece[:, None], ("kv", "tp"), axis=1, tiled=True),
        lax.all_gather(column_piece[:, None], ("kv", "tp"), axis=1, tiled=True),
    )
    rank_slice = query_latent.shape[2]
    all_latent = got_latent.reshape(seq_count, kv_count, tp_count, heads_dev, rank_slice)
    all_latent = all_latent.transpose(0, 1, 3, 2, 4).reshape(seq_count, head_count, latent_rank)
    all_rope = got_rope.reshape(seq_count, kv_count, tp_count, heads_dev, rope_slice)
    all_rope = all_rope.transpose(0, 1, 3, 2, 4).reshape(seq_count, head_count, rope_width)
    fresh_f = got_columns.reshape(seq_count, latent_rank).astype(jnp.float32)
    new_latent = (
        fresh_f * lax.rsqrt(jnp.mean(fresh_f * fresh_f, axis=1, keepdims=True) + EPS) * latent_gain
    ).astype(jnp.bfloat16)
    new_latent_f = new_latent.astype(jnp.float32)
    own_score = (
        jnp.einsum("bhr,br->bh", all_latent, new_latent, preferred_element_type=jnp.float32)
        + jnp.einsum("bhq,bq->bh", all_rope, new_rotary, preferred_element_type=jnp.float32)
    ) * score_scale
    pos_dev = cache_latent.shape[1]
    first_pos = (kv_index * tp_count + tp_index) * pos_dev
    position = first_pos + jnp.arange(pos_dev, dtype=jnp.int32)
    valid = position[None, :] < lengths[:, None]
    scores = (
        jnp.einsum("bhr,bpr->bhp", all_latent, cache_latent, preferred_element_type=jnp.float32)
        + jnp.einsum("bhq,bpq->bhp", all_rope, cache_rotary, preferred_element_type=jnp.float32)
    ) * score_scale
    masked = jnp.where(valid[:, None, :], scores, -jnp.inf)
    local_top = jnp.maximum(jnp.max(masked, axis=2), own_score)
    top_score = lax.pmax(local_top, ("kv", "tp"))
    weights = jnp.where(valid[:, None, :], jnp.exp(scores - top_score[:, :, None]), 0.0)
    total_part = jnp.sum(weights, axis=2)
    summed_part = jnp.einsum(
        "bhp,bpr->bhr",
        weights.astype(jnp.bfloat16),
        cache_latent,
        preferred_element_type=jnp.float32,
    )
    own_weight = jnp.exp(own_score - top_score)
    block_own = lax.dynamic_slice_in_dim(own_weight, kv_index * heads_dev, heads_dev, 1)
    value_block_weight = lax.dynamic_slice_in_dim(w_value_up, kv_index * heads_dev, heads_dev, 1)
    totals, summed = lax.psum((total_part, summed_part), ("kv", "tp"))
    block_sum = lax.dynamic_slice_in_dim(summed, kv_index * heads_dev, heads_dev, 1)
    block_total = lax.dynamic_slice_in_dim(totals, kv_index * heads_dev, heads_dev, 1)
    latent_out = (block_sum + block_own[:, :, None] * new_latent_f[:, None, :]) / (
        block_total + block_own
    )[:, :, None]
    head_out = value_product(latent_out, value_block_weight).astype(jnp.bfloat16)
    out_part = jnp.dot(head_out.reshape(seq_count, -1), w_out, preferred_element_type=jnp.float32)
    mixed_out = lax.psum(out_part, "kv").astype(jnp.bfloat16)
    latent_width = latent_rank // (kv_count * tp_count)
    latent_piece = lax.dynamic_slice_in_dim(
        new_latent, (kv_index * tp_count + tp_index) * latent_width, latent_width, 1
    )
    return (mixed_out, latent_piece, new_rotary)


def solution(mesh):
    placed = (
        P(None, "tp"),
        P("tp"),
        P("tp", "kv", None),
        P("tp", "kv"),
        P("tp", None),
        P(),
        P("tp", "kv", None),
        P(),
        P("kv", "tp"),
        P(None, ("kv", "tp"), None),
        P(None, ("kv", "tp"), None),
        P(),
    )

    def step(*args):
        weights = (args[2], args[3], args[4], args[6], args[7], args[8])
        fits = fits_kernels(weights, mesh.shape["kv"], mesh.shape["tp"])
        return jax.shard_map(
            kernel_shards if fits else shards,
            mesh=mesh,
            in_specs=placed,
            out_specs=(P(None, "tp"), P(None, ("kv", "tp")), P()),
            check_vma=False,
        )(*args)

    return step
```

```python
import functools

import jax
import jax.numpy as jnp
from jax import lax
from jax.experimental import pallas as pl
from jax.experimental.pallas import tpu as pltpu
from jax.sharding import PartitionSpec as P

MESH = pl.DeviceIdType.MESH
LANES = 128
INNER = 2
LOWEST = -1e38

THETA = 10000.0
EPS = 1e-06


def rotate(values, position):
    full_width = values.shape[-1]
    half_width = full_width // 2
    frequency = THETA ** (-jnp.arange(0, full_width, 2, dtype=jnp.float32) / full_width)
    angles = position.astype(jnp.float32)[:, None] * frequency[None, :]
    angles = angles.reshape((angles.shape[0],) + (1,) * (values.ndim - 2) + (half_width,))
    cosine = jnp.cos(angles)
    sine_part = jnp.sin(angles)
    first_half = values[..., :half_width]
    second_half = values[..., half_width:]
    return jnp.concatenate(
        [
            first_half * cosine - second_half * sine_part,
            first_half * sine_part + second_half * cosine,
        ],
        axis=-1,
    )


def value_product(latent_f, weight):
    high_part = latent_f.astype(jnp.bfloat16)
    low_part = (latent_f - high_part.astype(jnp.float32)).astype(jnp.bfloat16)
    return jnp.einsum(
        "bhr,rhv->bhv", high_part, weight, preferred_element_type=jnp.float32
    ) + jnp.einsum("bhr,rhv->bhv", low_part, weight, preferred_element_type=jnp.float32)


def greet(peers):
    barrier = pltpu.get_barrier_semaphore()
    for peer in peers:
        pl.semaphore_signal(barrier, inc=1, device_id=peer, device_id_type=MESH)
    pl.semaphore_wait(barrier, len(peers))


def remote(source, target, send, recv, peer):
    return pltpu.make_async_remote_copy(
        src_ref=source,
        dst_ref=target,
        send_sem=send,
        recv_sem=recv,
        device_id=peer,
        device_id_type=MESH,
    )


def tp_sum_kernel(tp_count, part_ref, sum_ref, slots, send, recv):
    kv_index, tp_index = lax.axis_index("kv"), lax.axis_index("tp")
    peers = [(kv_index, lax.rem(tp_index + step, tp_count)) for step in range(1, tp_count)]
    greet(peers)
    copies = []
    for step, peer in enumerate(peers):
        copies.append(
            remote(part_ref, slots.at[tp_index], send.at[step], recv.at[step], peer)
        )
        copies[-1].start()
    slots[tp_index] = part_ref[...]
    for copy in copies:
        copy.wait()
    sum_ref[...] = jnp.sum(slots[...], axis=0)


def tp_sum(part, tp_count):
    return pl.pallas_call(
        functools.partial(tp_sum_kernel, tp_count),
        out_shape=jax.ShapeDtypeStruct(part.shape, part.dtype),
        in_specs=[pl.BlockSpec(memory_space=pltpu.VMEM)],
        out_specs=pl.BlockSpec(memory_space=pltpu.VMEM),
        scratch_shapes=[
            pltpu.VMEM((tp_count,) + part.shape, part.dtype),
            pltpu.SemaphoreType.DMA((tp_count - 1,)),
            pltpu.SemaphoreType.DMA((tp_count - 1,)),
        ],
        compiler_params=pltpu.CompilerParams(collective_id=0, has_side_effects=True),
        name="tp_sum",
    )(part)


def plane_offsets(tp_count):
    return [(inner, step) for inner in range(INNER) for step in range(0, tp_count, 2)]


def plane_peer(kv_index, tp_index, tp_count, offset):
    outer, inner = kv_index // INNER, lax.rem(kv_index, INNER)
    return (
        outer * INNER + lax.rem(inner + offset[0], INNER),
        lax.rem(tp_index + offset[1], tp_count),
    )


def sibling_of(tp_index):
    return tp_index + 1 - 2 * lax.rem(tp_index, 2)


def gather_kernel(
    kv_count,
    tp_count,
    query_ref,
    extra_ref,
    query_out,
    extra_out,
    query_all,
    extra_all,
    line_send,
    line_recv,
    plane_send,
    plane_recv,
    pair_send,
    pair_recv,
    extra_send,
    extra_recv,
    side_send,
    side_recv,
):
    kv_index, tp_index = lax.axis_index("kv"), lax.axis_index("tp")
    heads, _, width = query_ref.shape
    lines = kv_count // INNER
    offsets = plane_offsets(tp_count)
    back = [(-inner % INNER, -step % tp_count) for inner, step in offsets]
    sibling = (kv_index, sibling_of(tp_index))
    line_peers = [
        (lax.rem(kv_index + INNER * step, kv_count), tp_index) for step in range(1, lines)
    ]
    planes = [plane_peer(kv_index, tp_index, tp_count, offset) for offset in offsets]
    sources = [plane_peer(kv_index, tp_index, tp_count, offset) for offset in back]
    greet(line_peers + planes[1:] + [sibling])

    def shifted(kv_at, step):
        return lax.rem(kv_at - INNER * step + kv_count, kv_count)

    def place(kv_at, tp_at):
        return query_all.at[
            pl.ds(pl.multiple_of(kv_at * heads, heads), heads),
            :,
            pl.ds(pl.multiple_of(tp_at * width, LANES), width),
        ]

    copies, line_copies, extra_copies, plane_copies = [], [], [], {}
    mine = place(kv_index, tp_index)
    for step, peer in enumerate(line_peers):
        line_copies.append(remote(query_ref, mine, line_send.at[step], line_recv.at[step], peer))
        line_copies[-1].start()
        extra_copies.append(
            remote(
                extra_ref, extra_all.at[kv_index], extra_send.at[step], extra_recv.at[step], peer
            )
        )
        extra_copies[-1].start()
    query_all[
        pl.ds(pl.multiple_of(kv_index * heads, heads), heads),
        :,
        pl.ds(pl.multiple_of(tp_index * width, LANES), width),
    ] = query_ref[...]
    extra_all[kv_index] = extra_ref[...]

    side = plane_peer(kv_index, tp_index, tp_count, (1, 0))
    side_copies = []
    for line in range(lines):
        kv_at = shifted(kv_index, line)
        target = place(kv_at, tp_index)
        extra_target = extra_all.at[kv_at]
        if line > 0:
            line_copies[line - 1].wait_recv()
            extra_copies[line - 1].wait_recv()
        for slot in range(1, len(offsets)):
            plane_copies[line, slot] = remote(
                query_ref if line == 0 else target,
                target,
                plane_send.at[line, slot],
                plane_recv.at[line, slot],
                planes[slot],
            )
            plane_copies[line, slot].start()
        side_copies.append(
            remote(
                extra_ref if line == 0 else extra_target,
                extra_target,
                side_send.at[line],
                side_recv.at[line],
                side,
            )
        )
        side_copies[-1].start()
        copies.append(
            remote(
                query_ref if line == 0 else target,
                target,
                pair_send.at[line, 0],
                pair_recv.at[line, 0],
                sibling,
            )
        )
        copies[-1].start()
    for line in range(lines):
        for slot in range(1, len(offsets)):
            plane_copies[line, slot].wait_recv()
            target = place(shifted(sources[slot][0], line), sources[slot][1])
            copies.append(
                remote(
                    target, target, pair_send.at[line, slot], pair_recv.at[line, slot], sibling
                )
            )
            copies[-1].start()
    for copy in side_copies + copies:
        copy.wait()
    for copy in line_copies + extra_copies + list(plane_copies.values()):
        copy.wait_send()
    query_out[...] = query_all[...]
    extra_out[...] = extra_all[...]


def gather_all(query, extra, kv_count, tp_count):
    heads, seqs, width = query.shape
    query_shape = (heads * kv_count, seqs, width * tp_count)
    extra_shape = (kv_count,) + extra.shape
    lines, planes = kv_count // INNER, INNER * tp_count // 2
    return pl.pallas_call(
        functools.partial(gather_kernel, kv_count, tp_count),
        out_shape=(
            jax.ShapeDtypeStruct(query_shape, query.dtype),
            jax.ShapeDtypeStruct(extra_shape, extra.dtype),
        ),
        in_specs=[pl.BlockSpec(memory_space=pltpu.VMEM)] * 2,
        out_specs=(pl.BlockSpec(memory_space=pltpu.VMEM),) * 2,
        scratch_shapes=[
            pltpu.VMEM(query_shape, query.dtype),
            pltpu.VMEM(extra_shape, extra.dtype),
            pltpu.SemaphoreType.DMA((lines - 1,)),
            pltpu.SemaphoreType.DMA((lines - 1,)),
            pltpu.SemaphoreType.DMA((lines, planes)),
            pltpu.SemaphoreType.DMA((lines, planes)),
            pltpu.SemaphoreType.DMA((lines, planes)),
            pltpu.SemaphoreType.DMA((lines, planes)),
            pltpu.SemaphoreType.DMA((lines - 1,)),
            pltpu.SemaphoreType.DMA((lines - 1,)),
            pltpu.SemaphoreType.DMA((lines,)),
            pltpu.SemaphoreType.DMA((lines,)),
        ],
        compiler_params=pltpu.CompilerParams(collective_id=1, has_side_effects=True),
        name="gather_all",
    )(query, extra)


def split_stats(block, rank):
    values = block[:, :rank].astype(jnp.float32)
    stats = block[:, rank:].astype(jnp.float32)
    top = (stats[:, 0:1] + stats[:, 1:2]) + stats[:, 2:3]
    return values, top, stats[:, 3:4] + stats[:, 4:5]


def merge(first, second):
    values_a, top_a, total_a = first
    values_b, top_b, total_b = second
    top = jnp.maximum(top_a, top_b)
    scale_a, scale_b = jnp.exp(top_a - top), jnp.exp(top_b - top)
    return values_a * scale_a + values_b * scale_b, top, total_a * scale_a + total_b * scale_b


def rounded(value):
    return lax.reduce_precision(value, 8, 7)


def narrow(value):
    return value.astype(jnp.bfloat16).astype(jnp.float32)


def stats_lanes(top, total, lane, cut):
    high = cut(top)
    middle = cut(top - high)
    low = top - high - middle
    total_high = cut(total)
    total_low = total - total_high
    result = jnp.where(lane == 4, total_low, 0.0)
    for place, value in enumerate((high, middle, low, total_high)):
        result = jnp.where(lane == place, value, result)
    return result


def scatter_kernel(
    kv_count,
    tp_count,
    part_ref,
    own_ref,
    fresh_ref,
    value_ref,
    weight_ref,
    out_ref,
    from_pair,
    merged,
    from_plane,
    from_line,
    head_own,
    heads,
    parts,
    got,
    done,
    final,
    pair_send,
    pair_recv,
    plane_send,
    plane_recv,
    line_send,
    line_recv,
    head_send,
    head_recv,
    part_send,
    part_recv,
    done_send,
    done_recv,
):
    kv_index, tp_index = lax.axis_index("kv"), lax.axis_index("tp")
    seqs, rank = fresh_ref.shape
    lane = lax.broadcasted_iota(jnp.int32, (seqs, LANES), 1)
    lines = kv_count // INNER
    offsets = plane_offsets(tp_count)
    sibling = (kv_index, sibling_of(tp_index))
    planes = [plane_peer(kv_index, tp_index, tp_count, offset) for offset in offsets]
    crossed = [plane for plane, offset in zip(planes, offsets) if offset[0] > 0 and offset[1] > 0]
    tp_peers = [(kv_index, lax.rem(tp_index + step, tp_count)) for step in range(1, tp_count)]
    kv_peers = [(lax.rem(kv_index + step, kv_count), tp_index) for step in range(1, kv_count)]
    greet(tp_peers + kv_peers + crossed)

    def shifted(kv_at, step):
        return lax.rem(kv_at + INNER * step, kv_count)

    order = [(slot, line) for slot in range(len(offsets) - 1, 0, -1) for line in range(1, lines)]
    order += [(slot, 0) for slot in range(len(offsets) - 1, 0, -1)]
    order += [(0, line) for line in list(range(lines - 1, 0, -1)) + [0]]
    pair_copies, plane_copies, line_copies = {}, {}, {}
    for slot, line in order:
        kv_at, tp_at = shifted(planes[slot][0], line), planes[slot][1]
        pair_copies[slot, line] = remote(
            part_ref.at[kv_at * tp_count + sibling_of(tp_at)],
            from_pair.at[slot, line],
            pair_send.at[slot, line],
            pair_recv.at[slot, line],
            sibling,
        )
        pair_copies[slot, line].start()

    def put(slot, line, term):
        values, top, total = term
        merged[slot, line, :, :rank] = values.astype(merged.dtype)
        merged[slot, line, :, rank:] = stats_lanes(top, total, lane, narrow).astype(merged.dtype)

    own = None
    for slot, line in order:
        kv_at, tp_at = shifted(planes[slot][0], line), planes[slot][1]
        pair_copies[slot, line].wait_recv()
        term = merge(
            split_stats(part_ref[kv_at * tp_count + tp_at], rank),
            split_stats(from_pair[slot, line], rank),
        )
        if slot > 0:
            put(slot, line, term)
            plane_copies[slot, line] = remote(
                merged.at[slot, line],
                from_plane.at[slot, line],
                plane_send.at[slot, line],
                plane_recv.at[slot, line],
                planes[slot],
            )
            plane_copies[slot, line].start()
            continue
        for side in range(1, len(offsets)):
            plane_copies[side, line].wait_recv()
            term = merge(term, split_stats(from_plane[side, line], rank))
        if line == 0:
            own = term
            continue
        put(slot, line, term)
        line_copies[line] = remote(
            merged.at[slot, line],
            from_line.at[line],
            line_send.at[line],
            line_recv.at[line],
            (shifted(kv_index, line), tp_index),
        )
        line_copies[line].start()
    for line in range(1, lines):
        line_copies[line].wait_recv()
        own = merge(own, split_stats(from_line[line], rank))
    values, old_top, total = own
    own_score = own_ref[:, 0:1]
    top = jnp.maximum(old_top, own_score)
    old_scale, own_weight = jnp.exp(old_top - top), jnp.exp(own_score - top)
    latent_out = (values * old_scale + own_weight * fresh_ref[...].astype(jnp.float32)) / (
        total * old_scale + own_weight
    )
    high = latent_out.astype(jnp.bfloat16)
    low = (latent_out - high.astype(jnp.float32)).astype(jnp.bfloat16)
    head_out = jnp.dot(high, value_ref[...], preferred_element_type=jnp.float32) + jnp.dot(
        low, value_ref[...], preferred_element_type=jnp.float32
    )
    head_own[...] = head_out.astype(jnp.bfloat16)

    depth = head_own.shape[1]
    width = parts.shape[2]
    copies = []
    for step, peer in enumerate(tp_peers):
        copies.append(
            remote(head_own, heads.at[tp_index], head_send.at[step], head_recv.at[step], peer)
        )
        copies[-1].start()
    heads[tp_index] = head_own[...]
    for copy in copies:
        copy.wait()
    total = jnp.dot(heads[0], weight_ref[:depth, :], preferred_element_type=jnp.float32)
    for at in range(1, tp_count):
        total += jnp.dot(
            heads[at],
            weight_ref[at * depth : (at + 1) * depth, :],
            preferred_element_type=jnp.float32,
        )
    for at in range(kv_count):
        parts[at] = total[:, at * width : (at + 1) * width]
    copies = []
    for step, peer in enumerate(kv_peers):
        copies.append(
            remote(
                parts.at[peer[0]],
                got.at[kv_index],
                part_send.at[step],
                part_recv.at[step],
                peer,
            )
        )
        copies[-1].start()
    got[kv_index] = parts[kv_index]
    for copy in copies:
        copy.wait()
    mine = jnp.sum(got[...], axis=0).astype(out_ref.dtype)
    done[...] = mine
    copies = []
    for step, peer in enumerate(kv_peers):
        copies.append(
            remote(done, final.at[kv_index], done_send.at[step], done_recv.at[step], peer)
        )
        copies[-1].start()
    final[kv_index] = mine
    for copy in copies:
        copy.wait()
    for at in range(kv_count):
        out_ref[:, at * width : (at + 1) * width] = final[at]
    for copy in list(pair_copies.values()) + list(plane_copies.values()) + list(
        line_copies.values()
    ):
        copy.wait_send()


def scatter_project(part, own, fresh, value, weight, kv_count, tp_count):
    _, seqs, block = part.shape
    columns = weight.shape[1]
    width = columns // kv_count
    depth = value.shape[1]
    lines, planes = kv_count // INNER, INNER * tp_count // 2
    semaphores = [(planes, lines)] * 4 + [(lines,)] * 2
    semaphores += [(tp_count - 1,)] * 2 + [(kv_count - 1,)] * 4
    return pl.pallas_call(
        functools.partial(scatter_kernel, kv_count, tp_count),
        out_shape=jax.ShapeDtypeStruct((seqs, columns), jnp.bfloat16),
        in_specs=[pl.BlockSpec(memory_space=pltpu.VMEM)] * 5,
        out_specs=pl.BlockSpec(memory_space=pltpu.VMEM),
        scratch_shapes=[
            pltpu.VMEM((planes, lines, seqs, block), part.dtype),
            pltpu.VMEM((planes, lines, seqs, block), part.dtype),
            pltpu.VMEM((planes, lines, seqs, block), part.dtype),
            pltpu.VMEM((lines, seqs, block), part.dtype),
            pltpu.VMEM((seqs, depth), jnp.bfloat16),
            pltpu.VMEM((tp_count, seqs, depth), jnp.bfloat16),
            pltpu.VMEM((kv_count, seqs, width), jnp.float32),
            pltpu.VMEM((kv_count, seqs, width), jnp.float32),
            pltpu.VMEM((seqs, width), jnp.bfloat16),
            pltpu.VMEM((kv_count, seqs, width), jnp.bfloat16),
        ]
        + [pltpu.SemaphoreType.DMA(shape) for shape in semaphores],
        compiler_params=pltpu.CompilerParams(collective_id=2, has_side_effects=True),
        name="scatter_project",
    )(part, own, fresh, value, weight)


def kernel_shards(
    tokens,
    norm_gain,
    w_query,
    w_latent,
    w_rotary,
    latent_gain,
    w_key_up,
    w_value_up,
    w_out,
    cache_latent,
    cache_rotary,
    lengths,
):
    seq_count = tokens.shape[0]
    kv_count = lax.axis_size("kv")
    tp_count = lax.axis_size("tp")
    kv_index = lax.axis_index("kv")
    tp_index = lax.axis_index("tp")
    device = kv_index * tp_count + tp_index
    heads_dev = w_query.shape[1]
    head_count = heads_dev * kv_count
    latent_rank = cache_latent.shape[2]
    rope_width = cache_rotary.shape[2]
    nope_width = w_query.shape[2] - rope_width
    model_width = tokens.shape[1] * tp_count
    score_scale = w_query.shape[2] ** (-0.5)
    tokens_f = tokens.astype(jnp.float32)
    scaled = (tokens_f * norm_gain).astype(jnp.bfloat16)
    query_part = jnp.einsum("bd,dhn->bhn", scaled, w_query, preferred_element_type=jnp.float32)
    latent_part = jnp.dot(scaled, w_latent, preferred_element_type=jnp.float32)
    rotary_part = jnp.dot(scaled, w_rotary, preferred_element_type=jnp.float32)
    square_part = jnp.sum(tokens_f * tokens_f, axis=1)
    query_width = heads_dev * w_query.shape[2]
    latent_width = latent_part.shape[1]
    fill = -(query_width + latent_width + rope_width) % LANES or LANES
    packed = jnp.concatenate(
        [
            query_part.reshape(seq_count, query_width),
            latent_part,
            rotary_part,
            jnp.broadcast_to(square_part[:, None], (seq_count, fill)),
        ],
        axis=1,
    )
    packed = tp_sum(packed, tp_count)
    query_sum, latent_sum, rotary_sum, square_sum = jnp.split(
        packed,
        [query_width, query_width + latent_width, query_width + latent_width + rope_width],
        axis=1,
    )
    inverse = lax.rsqrt(square_sum[:, :1] / model_width + EPS)
    query_heads = (query_sum * inverse).astype(jnp.bfloat16)
    query_heads = query_heads.reshape(seq_count, heads_dev, w_query.shape[2])
    compressed = (latent_sum * inverse).astype(jnp.bfloat16)
    new_rotary = rotate(rotary_sum * inverse, lengths).astype(jnp.bfloat16)
    query_rope = rotate(query_heads[:, :, nope_width:].astype(jnp.float32), lengths).astype(
        jnp.bfloat16
    )
    query_latent = jnp.einsum(
        "bhn,rhn->hbr", query_heads[:, :, :nope_width], w_key_up, preferred_element_type=jnp.float32
    ).astype(jnp.bfloat16)
    rope_flat = query_rope.reshape(seq_count, heads_dev * rope_width)
    got_latent, got_extra = gather_all(
        query_latent, jnp.concatenate([rope_flat, compressed], axis=1), kv_count, tp_count
    )
    all_latent = got_latent.transpose(1, 0, 2)
    all_rope = got_extra[:, :, : heads_dev * rope_width]
    all_rope = all_rope.reshape(kv_count, seq_count, heads_dev, rope_width)
    all_rope = all_rope.transpose(1, 0, 2, 3).reshape(seq_count, head_count, rope_width)
    fresh_f = got_extra[:, :, heads_dev * rope_width :].transpose(1, 0, 2)
    fresh_f = fresh_f.reshape(seq_count, latent_rank).astype(jnp.float32)
    new_latent = (
        fresh_f * lax.rsqrt(jnp.mean(fresh_f * fresh_f, axis=1, keepdims=True) + EPS) * latent_gain
    ).astype(jnp.bfloat16)
    own_query = lax.dynamic_slice_in_dim(got_latent, device, 1, 0)[0].astype(jnp.float32)
    own_rope = lax.dynamic_slice_in_dim(all_rope, device, 1, 1)[:, 0].astype(jnp.float32)
    own = (
        jnp.sum(own_query * new_latent.astype(jnp.float32), axis=1, keepdims=True)
        + jnp.sum(own_rope * new_rotary.astype(jnp.float32), axis=1, keepdims=True)
    ) * score_scale
    own = jnp.broadcast_to(own, (seq_count, LANES))
    pos_dev = cache_latent.shape[1]
    position = device * pos_dev + jnp.arange(pos_dev, dtype=jnp.int32)
    valid = position[None, :] < lengths[:, None]
    scores = (
        jnp.einsum("bhr,bpr->bhp", all_latent, cache_latent, preferred_element_type=jnp.float32)
        + jnp.einsum("bhq,bpq->bhp", all_rope, cache_rotary, preferred_element_type=jnp.float32)
    ) * score_scale
    masked = jnp.where(valid[:, None, :], scores, -jnp.inf)
    local_top = jnp.maximum(jnp.max(masked, axis=2), LOWEST)
    weights = jnp.where(valid[:, None, :], jnp.exp(scores - local_top[:, :, None]), 0.0)
    total_part = jnp.sum(weights, axis=2)
    summed_part = jnp.einsum(
        "bhp,bpr->bhr",
        weights.astype(jnp.bfloat16),
        cache_latent,
        preferred_element_type=jnp.float32,
    ).astype(jnp.bfloat16)
    lane = lax.broadcasted_iota(jnp.int32, (seq_count, head_count, LANES), 2)
    stats = stats_lanes(local_top[:, :, None], total_part[:, :, None], lane, rounded)
    part = jnp.concatenate([summed_part, stats.astype(jnp.bfloat16)], axis=2).transpose(1, 0, 2)
    value_weight = lax.dynamic_slice_in_dim(w_value_up, device, 1, 1)[:, 0, :]
    mixed_out = scatter_project(part, own, new_latent, value_weight, w_out, kv_count, tp_count)
    piece_width = latent_rank // (kv_count * tp_count)
    latent_piece = lax.dynamic_slice_in_dim(new_latent, device * piece_width, piece_width, 1)
    return (mixed_out, latent_piece, new_rotary)


def fits_kernels(args, kv_count, tp_count):
    w_query, w_latent, w_rotary, w_key_up, w_value_up, w_out = args
    heads = w_query.shape[1]
    return (
        heads == kv_count * tp_count
        and tp_count % 2 == 0
        and kv_count % INNER == 0
        and kv_count > INNER
        and w_key_up.shape[0] // tp_count % LANES == 0
        and w_latent.shape[1] // kv_count % LANES == 0
        and heads // kv_count * w_rotary.shape[1] % LANES == 0
        and w_value_up.shape[2] % LANES == 0
        and w_out.shape[1] // tp_count // kv_count % LANES == 0
    )


def shards(
    tokens,
    norm_gain,
    w_query,
    w_latent,
    w_rotary,
    latent_gain,
    w_key_up,
    w_value_up,
    w_out,
    cache_latent,
    cache_rotary,
    lengths,
):
    seq_count = tokens.shape[0]
    kv_count = lax.axis_size("kv")
    tp_count = lax.axis_size("tp")
    kv_index = lax.axis_index("kv")
    tp_index = lax.axis_index("tp")
    heads_dev = w_query.shape[1]
    head_count = heads_dev * kv_count
    latent_rank = cache_latent.shape[2]
    rope_width = cache_rotary.shape[2]
    nope_width = w_query.shape[2] - rope_width
    model_width = tokens.shape[1] * tp_count
    score_scale = w_query.shape[2] ** (-0.5)
    tokens_f = tokens.astype(jnp.float32)
    scaled = (tokens_f * norm_gain).astype(jnp.bfloat16)
    query_part = jnp.einsum("bd,dhn->bhn", scaled, w_query, preferred_element_type=jnp.float32)
    latent_part = jnp.dot(scaled, w_latent, preferred_element_type=jnp.float32)
    rotary_part = jnp.dot(scaled, w_rotary, preferred_element_type=jnp.float32)
    square_part = jnp.sum(tokens_f * tokens_f, axis=1)
    query_sum, latent_sum, rotary_sum, square_sum = lax.psum(
        (query_part, latent_part, rotary_part, square_part), "tp"
    )
    inverse = lax.rsqrt(square_sum / model_width + EPS)
    query_heads = (query_sum * inverse[:, None, None]).astype(jnp.bfloat16)
    compressed = (latent_sum * inverse[:, None]).astype(jnp.bfloat16)
    new_rotary = rotate(rotary_sum * inverse[:, None], lengths).astype(jnp.bfloat16)
    query_rope = rotate(query_heads[:, :, nope_width:].astype(jnp.float32), lengths).astype(
        jnp.bfloat16
    )
    query_latent = jnp.einsum(
        "bhn,rhn->bhr", query_heads[:, :, :nope_width], w_key_up, preferred_element_type=jnp.float32
    ).astype(jnp.bfloat16)
    rope_slice = rope_width // tp_count
    column_slice = compressed.shape[1] // tp_count
    rope_piece = lax.dynamic_slice_in_dim(query_rope, tp_index * rope_slice, rope_slice, 2)
    column_piece = lax.dynamic_slice_in_dim(compressed, tp_index * column_slice, column_slice, 1)
    got_latent, got_rope, got_columns = (
        lax.all_gather(query_latent[:, None], ("kv", "tp"), axis=1, tiled=True),
        lax.all_gather(rope_piece[:, None], ("kv", "tp"), axis=1, tiled=True),
        lax.all_gather(column_piece[:, None], ("kv", "tp"), axis=1, tiled=True),
    )
    rank_slice = query_latent.shape[2]
    all_latent = got_latent.reshape(seq_count, kv_count, tp_count, heads_dev, rank_slice)
    all_latent = all_latent.transpose(0, 1, 3, 2, 4).reshape(seq_count, head_count, latent_rank)
    all_rope = got_rope.reshape(seq_count, kv_count, tp_count, heads_dev, rope_slice)
    all_rope = all_rope.transpose(0, 1, 3, 2, 4).reshape(seq_count, head_count, rope_width)
    fresh_f = got_columns.reshape(seq_count, latent_rank).astype(jnp.float32)
    new_latent = (
        fresh_f * lax.rsqrt(jnp.mean(fresh_f * fresh_f, axis=1, keepdims=True) + EPS) * latent_gain
    ).astype(jnp.bfloat16)
    new_latent_f = new_latent.astype(jnp.float32)
    own_score = (
        jnp.einsum("bhr,br->bh", all_latent, new_latent, preferred_element_type=jnp.float32)
        + jnp.einsum("bhq,bq->bh", all_rope, new_rotary, preferred_element_type=jnp.float32)
    ) * score_scale
    pos_dev = cache_latent.shape[1]
    first_pos = (kv_index * tp_count + tp_index) * pos_dev
    position = first_pos + jnp.arange(pos_dev, dtype=jnp.int32)
    valid = position[None, :] < lengths[:, None]
    scores = (
        jnp.einsum("bhr,bpr->bhp", all_latent, cache_latent, preferred_element_type=jnp.float32)
        + jnp.einsum("bhq,bpq->bhp", all_rope, cache_rotary, preferred_element_type=jnp.float32)
    ) * score_scale
    masked = jnp.where(valid[:, None, :], scores, -jnp.inf)
    local_top = jnp.maximum(jnp.max(masked, axis=2), own_score)
    top_score = lax.pmax(local_top, ("kv", "tp"))
    weights = jnp.where(valid[:, None, :], jnp.exp(scores - top_score[:, :, None]), 0.0)
    total_part = jnp.sum(weights, axis=2)
    summed_part = jnp.einsum(
        "bhp,bpr->bhr",
        weights.astype(jnp.bfloat16),
        cache_latent,
        preferred_element_type=jnp.float32,
    )
    own_weight = jnp.exp(own_score - top_score)
    block_own = lax.dynamic_slice_in_dim(own_weight, kv_index * heads_dev, heads_dev, 1)
    value_block_weight = lax.dynamic_slice_in_dim(w_value_up, kv_index * heads_dev, heads_dev, 1)
    totals, summed = lax.psum((total_part, summed_part), ("kv", "tp"))
    block_sum = lax.dynamic_slice_in_dim(summed, kv_index * heads_dev, heads_dev, 1)
    block_total = lax.dynamic_slice_in_dim(totals, kv_index * heads_dev, heads_dev, 1)
    latent_out = (block_sum + block_own[:, :, None] * new_latent_f[:, None, :]) / (
        block_total + block_own
    )[:, :, None]
    head_out = value_product(latent_out, value_block_weight).astype(jnp.bfloat16)
    out_part = jnp.dot(head_out.reshape(seq_count, -1), w_out, preferred_element_type=jnp.float32)
    mixed_out = lax.psum(out_part, "kv").astype(jnp.bfloat16)
    latent_width = latent_rank // (kv_count * tp_count)
    latent_piece = lax.dynamic_slice_in_dim(
        new_latent, (kv_index * tp_count + tp_index) * latent_width, latent_width, 1
    )
    return (mixed_out, latent_piece, new_rotary)


def solution(mesh):
    placed = (
        P(None, "tp"),
        P("tp"),
        P("tp", "kv", None),
        P("tp", "kv"),
        P("tp", None),
        P(),
        P("tp", "kv", None),
        P(),
        P("kv", "tp"),
        P(None, ("kv", "tp"), None),
        P(None, ("kv", "tp"), None),
        P(),
    )

    def step(*args):
        weights = (args[2], args[3], args[4], args[6], args[7], args[8])
        fits = fits_kernels(weights, mesh.shape["kv"], mesh.shape["tp"])
        return jax.shard_map(
            kernel_shards if fits else shards,
            mesh=mesh,
            in_specs=placed,
            out_specs=(P(None, "tp"), P(None, ("kv", "tp")), P()),
            check_vma=False,
        )(*args)

    return step
```

```python
import functools

import jax
import jax.numpy as jnp
from jax import lax
from jax.experimental import pallas as pl
from jax.experimental.pallas import tpu as pltpu
from jax.sharding import PartitionSpec as P

MESH = pl.DeviceIdType.MESH
LANES = 128
INNER = 2
LOWEST = -1e38

THETA = 10000.0
EPS = 1e-06


def rotate(values, position):
    full_width = values.shape[-1]
    half_width = full_width // 2
    frequency = THETA ** (-jnp.arange(0, full_width, 2, dtype=jnp.float32) / full_width)
    angles = position.astype(jnp.float32)[:, None] * frequency[None, :]
    angles = angles.reshape((angles.shape[0],) + (1,) * (values.ndim - 2) + (half_width,))
    cosine = jnp.cos(angles)
    sine_part = jnp.sin(angles)
    first_half = values[..., :half_width]
    second_half = values[..., half_width:]
    return jnp.concatenate(
        [
            first_half * cosine - second_half * sine_part,
            first_half * sine_part + second_half * cosine,
        ],
        axis=-1,
    )


def value_product(latent_f, weight):
    high_part = latent_f.astype(jnp.bfloat16)
    low_part = (latent_f - high_part.astype(jnp.float32)).astype(jnp.bfloat16)
    return jnp.einsum(
        "bhr,rhv->bhv", high_part, weight, preferred_element_type=jnp.float32
    ) + jnp.einsum("bhr,rhv->bhv", low_part, weight, preferred_element_type=jnp.float32)


def greet(peers):
    barrier = pltpu.get_barrier_semaphore()
    for peer in peers:
        pl.semaphore_signal(barrier, inc=1, device_id=peer, device_id_type=MESH)
    pl.semaphore_wait(barrier, len(peers))


def remote(source, target, send, recv, peer):
    return pltpu.make_async_remote_copy(
        src_ref=source,
        dst_ref=target,
        send_sem=send,
        recv_sem=recv,
        device_id=peer,
        device_id_type=MESH,
    )


def tp_sum_kernel(
    tp_count, model_width, square_at, part_ref, query_ref, latent_ref, rest_ref, slots, send, recv
):
    kv_index, tp_index = lax.axis_index("kv"), lax.axis_index("tp")
    peers = [(kv_index, lax.rem(tp_index + step, tp_count)) for step in range(1, tp_count)]
    greet(peers)
    copies = []
    for step, peer in enumerate(peers):
        copies.append(
            remote(part_ref, slots.at[tp_index], send.at[step], recv.at[step], peer)
        )
        copies[-1].start()
    slots[tp_index] = part_ref[...]
    for copy in copies:
        copy.wait()
    total = jnp.sum(slots[...], axis=0)
    total = total * lax.rsqrt(total[:, square_at : square_at + 1] / model_width + EPS)
    query_width = query_ref.shape[1]
    rest_at = query_width + latent_ref.shape[1]
    query_ref[...] = total[:, :query_width].astype(query_ref.dtype)
    latent_ref[...] = total[:, query_width:rest_at].astype(latent_ref.dtype)
    rest_ref[...] = total[:, rest_at:]


def tp_sum(part, tp_count, model_width, query_width, latent_width, rope_width):
    seqs, width = part.shape
    rest_at = query_width + latent_width
    return pl.pallas_call(
        functools.partial(tp_sum_kernel, tp_count, model_width, rest_at + rope_width),
        out_shape=(
            jax.ShapeDtypeStruct((seqs, query_width), jnp.bfloat16),
            jax.ShapeDtypeStruct((seqs, latent_width), jnp.bfloat16),
            jax.ShapeDtypeStruct((seqs, width - rest_at), jnp.float32),
        ),
        in_specs=[pl.BlockSpec(memory_space=pltpu.VMEM)],
        out_specs=(pl.BlockSpec(memory_space=pltpu.VMEM),) * 3,
        scratch_shapes=[
            pltpu.VMEM((tp_count,) + part.shape, part.dtype),
            pltpu.SemaphoreType.DMA((tp_count - 1,)),
            pltpu.SemaphoreType.DMA((tp_count - 1,)),
        ],
        compiler_params=pltpu.CompilerParams(collective_id=0, has_side_effects=True),
        name="tp_sum",
    )(part)


def plane_offsets(tp_count):
    return [(inner, step) for inner in range(INNER) for step in range(0, tp_count, 2)]


def plane_peer(kv_index, tp_index, tp_count, offset):
    outer, inner = kv_index // INNER, lax.rem(kv_index, INNER)
    return (
        outer * INNER + lax.rem(inner + offset[0], INNER),
        lax.rem(tp_index + offset[1], tp_count),
    )


def sibling_of(tp_index):
    return tp_index + 1 - 2 * lax.rem(tp_index, 2)


def gather_kernel(
    kv_count,
    tp_count,
    query_ref,
    extra_ref,
    query_out,
    extra_out,
    query_all,
    extra_all,
    line_send,
    line_recv,
    plane_send,
    plane_recv,
    pair_send,
    pair_recv,
    extra_send,
    extra_recv,
    side_send,
    side_recv,
):
    kv_index, tp_index = lax.axis_index("kv"), lax.axis_index("tp")
    heads, _, width = query_ref.shape
    lines = kv_count // INNER
    offsets = plane_offsets(tp_count)
    back = [(-inner % INNER, -step % tp_count) for inner, step in offsets]
    sibling = (kv_index, sibling_of(tp_index))
    line_peers = [
        (lax.rem(kv_index + INNER * step, kv_count), tp_index) for step in range(1, lines)
    ]
    planes = [plane_peer(kv_index, tp_index, tp_count, offset) for offset in offsets]
    sources = [plane_peer(kv_index, tp_index, tp_count, offset) for offset in back]
    greet(line_peers + planes[1:] + [sibling])

    def shifted(kv_at, step):
        return lax.rem(kv_at - INNER * step + kv_count, kv_count)

    def place(kv_at, tp_at):
        return query_all.at[
            pl.ds(pl.multiple_of(kv_at * heads, heads), heads),
            :,
            pl.ds(pl.multiple_of(tp_at * width, LANES), width),
        ]

    copies, line_copies, extra_copies, plane_copies = [], [], [], {}
    mine = place(kv_index, tp_index)
    for step, peer in enumerate(line_peers):
        line_copies.append(remote(query_ref, mine, line_send.at[step], line_recv.at[step], peer))
        line_copies[-1].start()
        extra_copies.append(
            remote(
                extra_ref, extra_all.at[kv_index], extra_send.at[step], extra_recv.at[step], peer
            )
        )
        extra_copies[-1].start()
    query_all[
        pl.ds(pl.multiple_of(kv_index * heads, heads), heads),
        :,
        pl.ds(pl.multiple_of(tp_index * width, LANES), width),
    ] = query_ref[...]
    extra_all[kv_index] = extra_ref[...]

    side = plane_peer(kv_index, tp_index, tp_count, (1, 0))
    side_copies = []
    for line in range(lines):
        kv_at = shifted(kv_index, line)
        target = place(kv_at, tp_index)
        extra_target = extra_all.at[kv_at]
        if line > 0:
            line_copies[line - 1].wait_recv()
            extra_copies[line - 1].wait_recv()
        for slot in range(1, len(offsets)):
            plane_copies[line, slot] = remote(
                query_ref if line == 0 else target,
                target,
                plane_send.at[line, slot],
                plane_recv.at[line, slot],
                planes[slot],
            )
            plane_copies[line, slot].start()
        side_copies.append(
            remote(
                extra_ref if line == 0 else extra_target,
                extra_target,
                side_send.at[line],
                side_recv.at[line],
                side,
            )
        )
        side_copies[-1].start()
        copies.append(
            remote(
                query_ref if line == 0 else target,
                target,
                pair_send.at[line, 0],
                pair_recv.at[line, 0],
                sibling,
            )
        )
        copies[-1].start()
    for line in range(lines):
        for slot in range(1, len(offsets)):
            plane_copies[line, slot].wait_recv()
            target = place(shifted(sources[slot][0], line), sources[slot][1])
            copies.append(
                remote(
                    target, target, pair_send.at[line, slot], pair_recv.at[line, slot], sibling
                )
            )
            copies[-1].start()
    for copy in side_copies + copies:
        copy.wait()
    for copy in line_copies + extra_copies + list(plane_copies.values()):
        copy.wait_send()
    query_out[...] = query_all[...]
    extra_out[...] = extra_all[...]


def gather_all(query, extra, kv_count, tp_count):
    heads, seqs, width = query.shape
    query_shape = (heads * kv_count, seqs, width * tp_count)
    extra_shape = (kv_count,) + extra.shape
    lines, planes = kv_count // INNER, INNER * tp_count // 2
    return pl.pallas_call(
        functools.partial(gather_kernel, kv_count, tp_count),
        out_shape=(
            jax.ShapeDtypeStruct(query_shape, query.dtype),
            jax.ShapeDtypeStruct(extra_shape, extra.dtype),
        ),
        in_specs=[pl.BlockSpec(memory_space=pltpu.VMEM)] * 2,
        out_specs=(pl.BlockSpec(memory_space=pltpu.VMEM),) * 2,
        scratch_shapes=[
            pltpu.VMEM(query_shape, query.dtype),
            pltpu.VMEM(extra_shape, extra.dtype),
            pltpu.SemaphoreType.DMA((lines - 1,)),
            pltpu.SemaphoreType.DMA((lines - 1,)),
            pltpu.SemaphoreType.DMA((lines, planes)),
            pltpu.SemaphoreType.DMA((lines, planes)),
            pltpu.SemaphoreType.DMA((lines, planes)),
            pltpu.SemaphoreType.DMA((lines, planes)),
            pltpu.SemaphoreType.DMA((lines - 1,)),
            pltpu.SemaphoreType.DMA((lines - 1,)),
            pltpu.SemaphoreType.DMA((lines,)),
            pltpu.SemaphoreType.DMA((lines,)),
        ],
        compiler_params=pltpu.CompilerParams(collective_id=1, has_side_effects=True),
        name="gather_all",
    )(query, extra)


def split_stats(block, rank):
    values = block[:, :rank].astype(jnp.float32)
    stats = block[:, rank:].astype(jnp.float32)
    top = (stats[:, 0:1] + stats[:, 1:2]) + stats[:, 2:3]
    return values, top, stats[:, 3:4] + stats[:, 4:5]


def merge(first, second):
    values_a, top_a, total_a = first
    values_b, top_b, total_b = second
    top = jnp.maximum(top_a, top_b)
    scale_a, scale_b = jnp.exp(top_a - top), jnp.exp(top_b - top)
    return values_a * scale_a + values_b * scale_b, top, total_a * scale_a + total_b * scale_b


def rounded(value):
    return lax.reduce_precision(value, 8, 7)


def narrow(value):
    return value.astype(jnp.bfloat16).astype(jnp.float32)


def stats_lanes(top, total, lane, cut):
    high = cut(top)
    middle = cut(top - high)
    low = top - high - middle
    total_high = cut(total)
    total_low = total - total_high
    result = jnp.where(lane == 4, total_low, 0.0)
    for place, value in enumerate((high, middle, low, total_high)):
        result = jnp.where(lane == place, value, result)
    return result


def scatter_kernel(
    kv_count,
    tp_count,
    part_ref,
    own_ref,
    fresh_ref,
    value_ref,
    weight_ref,
    out_ref,
    from_pair,
    merged,
    from_plane,
    from_line,
    head_own,
    heads,
    parts,
    got,
    done,
    final,
    pair_send,
    pair_recv,
    plane_send,
    plane_recv,
    line_send,
    line_recv,
    head_send,
    head_recv,
    part_send,
    part_recv,
    done_send,
    done_recv,
):
    kv_index, tp_index = lax.axis_index("kv"), lax.axis_index("tp")
    seqs, rank = fresh_ref.shape
    lane = lax.broadcasted_iota(jnp.int32, (seqs, LANES), 1)
    lines = kv_count // INNER
    offsets = plane_offsets(tp_count)
    sibling = (kv_index, sibling_of(tp_index))
    planes = [plane_peer(kv_index, tp_index, tp_count, offset) for offset in offsets]
    crossed = [plane for plane, offset in zip(planes, offsets) if offset[0] > 0 and offset[1] > 0]
    tp_peers = [(kv_index, lax.rem(tp_index + step, tp_count)) for step in range(1, tp_count)]
    kv_peers = [(lax.rem(kv_index + step, kv_count), tp_index) for step in range(1, kv_count)]
    greet(tp_peers + kv_peers + crossed)

    def shifted(kv_at, step):
        return lax.rem(kv_at + INNER * step, kv_count)

    order = [(slot, line) for slot in range(len(offsets) - 1, 0, -1) for line in range(1, lines)]
    order += [(slot, 0) for slot in range(len(offsets) - 1, 0, -1)]
    order += [(0, line) for line in list(range(lines - 1, 0, -1)) + [0]]
    pair_copies, plane_copies, line_copies = {}, {}, {}
    for slot, line in order:
        kv_at, tp_at = shifted(planes[slot][0], line), planes[slot][1]
        pair_copies[slot, line] = remote(
            part_ref.at[kv_at * tp_count + sibling_of(tp_at)],
            from_pair.at[slot, line],
            pair_send.at[slot, line],
            pair_recv.at[slot, line],
            sibling,
        )
        pair_copies[slot, line].start()

    def put(slot, line, term):
        values, top, total = term
        merged[slot, line, :, :rank] = values.astype(merged.dtype)
        merged[slot, line, :, rank:] = stats_lanes(top, total, lane, narrow).astype(merged.dtype)

    own = None
    for slot, line in order:
        kv_at, tp_at = shifted(planes[slot][0], line), planes[slot][1]
        pair_copies[slot, line].wait_recv()
        term = merge(
            split_stats(part_ref[kv_at * tp_count + tp_at], rank),
            split_stats(from_pair[slot, line], rank),
        )
        if slot > 0:
            put(slot, line, term)
            plane_copies[slot, line] = remote(
                merged.at[slot, line],
                from_plane.at[slot, line],
                plane_send.at[slot, line],
                plane_recv.at[slot, line],
                planes[slot],
            )
            plane_copies[slot, line].start()
            continue
        for side in range(1, len(offsets)):
            plane_copies[side, line].wait_recv()
            term = merge(term, split_stats(from_plane[side, line], rank))
        if line == 0:
            own = term
            continue
        put(slot, line, term)
        line_copies[line] = remote(
            merged.at[slot, line],
            from_line.at[line],
            line_send.at[line],
            line_recv.at[line],
            (shifted(kv_index, line), tp_index),
        )
        line_copies[line].start()
    for line in range(1, lines):
        line_copies[line].wait_recv()
        own = merge(own, split_stats(from_line[line], rank))
    values, old_top, total = own
    own_score = own_ref[:, 0:1]
    top = jnp.maximum(old_top, own_score)
    old_scale, own_weight = jnp.exp(old_top - top), jnp.exp(own_score - top)
    latent_out = (values * old_scale + own_weight * fresh_ref[...].astype(jnp.float32)) / (
        total * old_scale + own_weight
    )
    high = latent_out.astype(jnp.bfloat16)
    low = (latent_out - high.astype(jnp.float32)).astype(jnp.bfloat16)
    head_out = jnp.dot(high, value_ref[...], preferred_element_type=jnp.float32) + jnp.dot(
        low, value_ref[...], preferred_element_type=jnp.float32
    )
    head_own[...] = head_out.astype(jnp.bfloat16)

    depth = head_own.shape[1]
    width = parts.shape[2]
    copies = []
    for step, peer in enumerate(tp_peers):
        copies.append(
            remote(head_own, heads.at[tp_index], head_send.at[step], head_recv.at[step], peer)
        )
        copies[-1].start()
    heads[tp_index] = head_own[...]
    for copy in copies:
        copy.wait()
    total = jnp.dot(heads[0], weight_ref[:depth, :], preferred_element_type=jnp.float32)
    for at in range(1, tp_count):
        total += jnp.dot(
            heads[at],
            weight_ref[at * depth : (at + 1) * depth, :],
            preferred_element_type=jnp.float32,
        )
    for at in range(kv_count):
        parts[at] = total[:, at * width : (at + 1) * width]
    copies = []
    for step, peer in enumerate(kv_peers):
        copies.append(
            remote(
                parts.at[peer[0]],
                got.at[kv_index],
                part_send.at[step],
                part_recv.at[step],
                peer,
            )
        )
        copies[-1].start()
    got[kv_index] = parts[kv_index]
    for copy in copies:
        copy.wait()
    mine = jnp.sum(got[...], axis=0).astype(out_ref.dtype)
    done[...] = mine
    copies = []
    for step, peer in enumerate(kv_peers):
        copies.append(
            remote(done, final.at[kv_index], done_send.at[step], done_recv.at[step], peer)
        )
        copies[-1].start()
    final[kv_index] = mine
    for copy in copies:
        copy.wait()
    for at in range(kv_count):
        out_ref[:, at * width : (at + 1) * width] = final[at]
    for copy in list(pair_copies.values()) + list(plane_copies.values()) + list(
        line_copies.values()
    ):
        copy.wait_send()


def scatter_project(part, own, fresh, value, weight, kv_count, tp_count):
    _, seqs, block = part.shape
    columns = weight.shape[1]
    width = columns // kv_count
    depth = value.shape[1]
    lines, planes = kv_count // INNER, INNER * tp_count // 2
    semaphores = [(planes, lines)] * 4 + [(lines,)] * 2
    semaphores += [(tp_count - 1,)] * 2 + [(kv_count - 1,)] * 4
    return pl.pallas_call(
        functools.partial(scatter_kernel, kv_count, tp_count),
        out_shape=jax.ShapeDtypeStruct((seqs, columns), jnp.bfloat16),
        in_specs=[pl.BlockSpec(memory_space=pltpu.VMEM)] * 5,
        out_specs=pl.BlockSpec(memory_space=pltpu.VMEM),
        scratch_shapes=[
            pltpu.VMEM((planes, lines, seqs, block), part.dtype),
            pltpu.VMEM((planes, lines, seqs, block), part.dtype),
            pltpu.VMEM((planes, lines, seqs, block), part.dtype),
            pltpu.VMEM((lines, seqs, block), part.dtype),
            pltpu.VMEM((seqs, depth), jnp.bfloat16),
            pltpu.VMEM((tp_count, seqs, depth), jnp.bfloat16),
            pltpu.VMEM((kv_count, seqs, width), jnp.float32),
            pltpu.VMEM((kv_count, seqs, width), jnp.float32),
            pltpu.VMEM((seqs, width), jnp.bfloat16),
            pltpu.VMEM((kv_count, seqs, width), jnp.bfloat16),
        ]
        + [pltpu.SemaphoreType.DMA(shape) for shape in semaphores],
        compiler_params=pltpu.CompilerParams(collective_id=2, has_side_effects=True),
        name="scatter_project",
    )(part, own, fresh, value, weight)


def kernel_shards(
    tokens,
    norm_gain,
    w_query,
    w_latent,
    w_rotary,
    latent_gain,
    w_key_up,
    w_value_up,
    w_out,
    cache_latent,
    cache_rotary,
    lengths,
):
    seq_count = tokens.shape[0]
    kv_count = lax.axis_size("kv")
    tp_count = lax.axis_size("tp")
    kv_index = lax.axis_index("kv")
    tp_index = lax.axis_index("tp")
    device = kv_index * tp_count + tp_index
    heads_dev = w_query.shape[1]
    head_count = heads_dev * kv_count
    latent_rank = cache_latent.shape[2]
    rope_width = cache_rotary.shape[2]
    nope_width = w_query.shape[2] - rope_width
    model_width = tokens.shape[1] * tp_count
    score_scale = w_query.shape[2] ** (-0.5)
    tokens_f = tokens.astype(jnp.float32)
    scaled = (tokens_f * norm_gain).astype(jnp.bfloat16)
    query_part = jnp.einsum("bd,dhn->bhn", scaled, w_query, preferred_element_type=jnp.float32)
    latent_part = jnp.dot(scaled, w_latent, preferred_element_type=jnp.float32)
    rotary_part = jnp.dot(scaled, w_rotary, preferred_element_type=jnp.float32)
    square_part = jnp.sum(tokens_f * tokens_f, axis=1)
    query_width = heads_dev * w_query.shape[2]
    latent_width = latent_part.shape[1]
    fill = -(query_width + latent_width + rope_width) % LANES or LANES
    packed = jnp.concatenate(
        [
            query_part.reshape(seq_count, query_width),
            latent_part,
            rotary_part,
            jnp.broadcast_to(square_part[:, None], (seq_count, fill)),
        ],
        axis=1,
    )
    query_heads, compressed, rest = tp_sum(
        packed, tp_count, model_width, query_width, latent_width, rope_width
    )
    query_heads = query_heads.reshape(seq_count, heads_dev, w_query.shape[2])
    new_rotary = rotate(rest[:, :rope_width], lengths).astype(jnp.bfloat16)
    query_rope = rotate(query_heads[:, :, nope_width:].astype(jnp.float32), lengths).astype(
        jnp.bfloat16
    )
    query_latent = jnp.einsum(
        "bhn,rhn->hbr", query_heads[:, :, :nope_width], w_key_up, preferred_element_type=jnp.float32
    ).astype(jnp.bfloat16)
    rope_flat = query_rope.reshape(seq_count, heads_dev * rope_width)
    got_latent, got_extra = gather_all(
        query_latent, jnp.concatenate([rope_flat, compressed], axis=1), kv_count, tp_count
    )
    all_latent = got_latent.transpose(1, 0, 2)
    all_rope = got_extra[:, :, : heads_dev * rope_width]
    all_rope = all_rope.reshape(kv_count, seq_count, heads_dev, rope_width)
    all_rope = all_rope.transpose(1, 0, 2, 3).reshape(seq_count, head_count, rope_width)
    fresh_f = got_extra[:, :, heads_dev * rope_width :].transpose(1, 0, 2)
    fresh_f = fresh_f.reshape(seq_count, latent_rank).astype(jnp.float32)
    new_latent = (
        fresh_f * lax.rsqrt(jnp.mean(fresh_f * fresh_f, axis=1, keepdims=True) + EPS) * latent_gain
    ).astype(jnp.bfloat16)
    own_query = lax.dynamic_slice_in_dim(got_latent, device, 1, 0)[0].astype(jnp.float32)
    own_rope = lax.dynamic_slice_in_dim(all_rope, device, 1, 1)[:, 0].astype(jnp.float32)
    own = (
        jnp.sum(own_query * new_latent.astype(jnp.float32), axis=1, keepdims=True)
        + jnp.sum(own_rope * new_rotary.astype(jnp.float32), axis=1, keepdims=True)
    ) * score_scale
    pos_dev = cache_latent.shape[1]
    position = device * pos_dev + jnp.arange(pos_dev, dtype=jnp.int32)
    valid = position[None, :] < lengths[:, None]
    scores = (
        jnp.einsum("bhr,bpr->bhp", all_latent, cache_latent, preferred_element_type=jnp.float32)
        + jnp.einsum("bhq,bpq->bhp", all_rope, cache_rotary, preferred_element_type=jnp.float32)
    ) * score_scale
    masked = jnp.where(valid[:, None, :], scores, -jnp.inf)
    local_top = jnp.maximum(jnp.max(masked, axis=2), LOWEST)
    weights = jnp.where(valid[:, None, :], jnp.exp(scores - local_top[:, :, None]), 0.0)
    total_part = jnp.sum(weights, axis=2)
    summed_part = jnp.einsum(
        "bhp,bpr->bhr",
        weights.astype(jnp.bfloat16),
        cache_latent,
        preferred_element_type=jnp.float32,
    ).astype(jnp.bfloat16)
    lane = lax.broadcasted_iota(jnp.int32, (seq_count, head_count, LANES), 2)
    stats = stats_lanes(local_top[:, :, None], total_part[:, :, None], lane, rounded)
    part = jnp.concatenate([summed_part, stats.astype(jnp.bfloat16)], axis=2).transpose(1, 0, 2)
    value_weight = lax.dynamic_slice_in_dim(w_value_up, device, 1, 1)[:, 0, :]
    mixed_out = scatter_project(part, own, new_latent, value_weight, w_out, kv_count, tp_count)
    piece_width = latent_rank // (kv_count * tp_count)
    latent_piece = lax.dynamic_slice_in_dim(new_latent, device * piece_width, piece_width, 1)
    return (mixed_out, latent_piece, new_rotary)


def fits_kernels(args, kv_count, tp_count):
    w_query, w_latent, w_rotary, w_key_up, w_value_up, w_out = args
    heads = w_query.shape[1]
    return (
        heads == kv_count * tp_count
        and tp_count % 2 == 0
        and kv_count % INNER == 0
        and kv_count > INNER
        and heads // kv_count * w_query.shape[2] % LANES == 0
        and w_key_up.shape[0] // tp_count % LANES == 0
        and w_latent.shape[1] // kv_count % LANES == 0
        and heads // kv_count * w_rotary.shape[1] % LANES == 0
        and w_value_up.shape[2] % LANES == 0
        and w_out.shape[1] // tp_count // kv_count % LANES == 0
    )


def shards(
    tokens,
    norm_gain,
    w_query,
    w_latent,
    w_rotary,
    latent_gain,
    w_key_up,
    w_value_up,
    w_out,
    cache_latent,
    cache_rotary,
    lengths,
):
    seq_count = tokens.shape[0]
    kv_count = lax.axis_size("kv")
    tp_count = lax.axis_size("tp")
    kv_index = lax.axis_index("kv")
    tp_index = lax.axis_index("tp")
    heads_dev = w_query.shape[1]
    head_count = heads_dev * kv_count
    latent_rank = cache_latent.shape[2]
    rope_width = cache_rotary.shape[2]
    nope_width = w_query.shape[2] - rope_width
    model_width = tokens.shape[1] * tp_count
    score_scale = w_query.shape[2] ** (-0.5)
    tokens_f = tokens.astype(jnp.float32)
    scaled = (tokens_f * norm_gain).astype(jnp.bfloat16)
    query_part = jnp.einsum("bd,dhn->bhn", scaled, w_query, preferred_element_type=jnp.float32)
    latent_part = jnp.dot(scaled, w_latent, preferred_element_type=jnp.float32)
    rotary_part = jnp.dot(scaled, w_rotary, preferred_element_type=jnp.float32)
    square_part = jnp.sum(tokens_f * tokens_f, axis=1)
    query_sum, latent_sum, rotary_sum, square_sum = lax.psum(
        (query_part, latent_part, rotary_part, square_part), "tp"
    )
    inverse = lax.rsqrt(square_sum / model_width + EPS)
    query_heads = (query_sum * inverse[:, None, None]).astype(jnp.bfloat16)
    compressed = (latent_sum * inverse[:, None]).astype(jnp.bfloat16)
    new_rotary = rotate(rotary_sum * inverse[:, None], lengths).astype(jnp.bfloat16)
    query_rope = rotate(query_heads[:, :, nope_width:].astype(jnp.float32), lengths).astype(
        jnp.bfloat16
    )
    query_latent = jnp.einsum(
        "bhn,rhn->bhr", query_heads[:, :, :nope_width], w_key_up, preferred_element_type=jnp.float32
    ).astype(jnp.bfloat16)
    rope_slice = rope_width // tp_count
    column_slice = compressed.shape[1] // tp_count
    rope_piece = lax.dynamic_slice_in_dim(query_rope, tp_index * rope_slice, rope_slice, 2)
    column_piece = lax.dynamic_slice_in_dim(compressed, tp_index * column_slice, column_slice, 1)
    got_latent, got_rope, got_columns = (
        lax.all_gather(query_latent[:, None], ("kv", "tp"), axis=1, tiled=True),
        lax.all_gather(rope_piece[:, None], ("kv", "tp"), axis=1, tiled=True),
        lax.all_gather(column_piece[:, None], ("kv", "tp"), axis=1, tiled=True),
    )
    rank_slice = query_latent.shape[2]
    all_latent = got_latent.reshape(seq_count, kv_count, tp_count, heads_dev, rank_slice)
    all_latent = all_latent.transpose(0, 1, 3, 2, 4).reshape(seq_count, head_count, latent_rank)
    all_rope = got_rope.reshape(seq_count, kv_count, tp_count, heads_dev, rope_slice)
    all_rope = all_rope.transpose(0, 1, 3, 2, 4).reshape(seq_count, head_count, rope_width)
    fresh_f = got_columns.reshape(seq_count, latent_rank).astype(jnp.float32)
    new_latent = (
        fresh_f * lax.rsqrt(jnp.mean(fresh_f * fresh_f, axis=1, keepdims=True) + EPS) * latent_gain
    ).astype(jnp.bfloat16)
    new_latent_f = new_latent.astype(jnp.float32)
    own_score = (
        jnp.einsum("bhr,br->bh", all_latent, new_latent, preferred_element_type=jnp.float32)
        + jnp.einsum("bhq,bq->bh", all_rope, new_rotary, preferred_element_type=jnp.float32)
    ) * score_scale
    pos_dev = cache_latent.shape[1]
    first_pos = (kv_index * tp_count + tp_index) * pos_dev
    position = first_pos + jnp.arange(pos_dev, dtype=jnp.int32)
    valid = position[None, :] < lengths[:, None]
    scores = (
        jnp.einsum("bhr,bpr->bhp", all_latent, cache_latent, preferred_element_type=jnp.float32)
        + jnp.einsum("bhq,bpq->bhp", all_rope, cache_rotary, preferred_element_type=jnp.float32)
    ) * score_scale
    masked = jnp.where(valid[:, None, :], scores, -jnp.inf)
    local_top = jnp.maximum(jnp.max(masked, axis=2), own_score)
    top_score = lax.pmax(local_top, ("kv", "tp"))
    weights = jnp.where(valid[:, None, :], jnp.exp(scores - top_score[:, :, None]), 0.0)
    total_part = jnp.sum(weights, axis=2)
    summed_part = jnp.einsum(
        "bhp,bpr->bhr",
        weights.astype(jnp.bfloat16),
        cache_latent,
        preferred_element_type=jnp.float32,
    )
    own_weight = jnp.exp(own_score - top_score)
    block_own = lax.dynamic_slice_in_dim(own_weight, kv_index * heads_dev, heads_dev, 1)
    value_block_weight = lax.dynamic_slice_in_dim(w_value_up, kv_index * heads_dev, heads_dev, 1)
    totals, summed = lax.psum((total_part, summed_part), ("kv", "tp"))
    block_sum = lax.dynamic_slice_in_dim(summed, kv_index * heads_dev, heads_dev, 1)
    block_total = lax.dynamic_slice_in_dim(totals, kv_index * heads_dev, heads_dev, 1)
    latent_out = (block_sum + block_own[:, :, None] * new_latent_f[:, None, :]) / (
        block_total + block_own
    )[:, :, None]
    head_out = value_product(latent_out, value_block_weight).astype(jnp.bfloat16)
    out_part = jnp.dot(head_out.reshape(seq_count, -1), w_out, preferred_element_type=jnp.float32)
    mixed_out = lax.psum(out_part, "kv").astype(jnp.bfloat16)
    latent_width = latent_rank // (kv_count * tp_count)
    latent_piece = lax.dynamic_slice_in_dim(
        new_latent, (kv_index * tp_count + tp_index) * latent_width, latent_width, 1
    )
    return (mixed_out, latent_piece, new_rotary)


def solution(mesh):
    placed = (
        P(None, "tp"),
        P("tp"),
        P("tp", "kv", None),
        P("tp", "kv"),
        P("tp", None),
        P(),
        P("tp", "kv", None),
        P(),
        P("kv", "tp"),
        P(None, ("kv", "tp"), None),
        P(None, ("kv", "tp"), None),
        P(),
    )

    def step(*args):
        weights = (args[2], args[3], args[4], args[6], args[7], args[8])
        fits = fits_kernels(weights, mesh.shape["kv"], mesh.shape["tp"])
        return jax.shard_map(
            kernel_shards if fits else shards,
            mesh=mesh,
            in_specs=placed,
            out_specs=(P(None, "tp"), P(None, ("kv", "tp")), P()),
            check_vma=False,
        )(*args)

    return step
```
